128 devices in a mesh: sp: 32 (over z, y, core), tp: 4 (over x).
Axes of the slice: x: 4, y: 4, z: 4, core: 2. Of those that a mesh axis runs over, the one named last changes fastest.
Arguments:
- conv_value: bfloat16 [16384, 2048], P('sp', 'tp'), may hold values from -6 to 6
- conv_gate: bfloat16 [16384, 2048], P('sp', 'tp'), may hold values from -6 to 6
- conv_taps: float32 [31, 2048], P(None, 'tp'), as said below
- channel_gain: float32 [2048], P('tp'), may hold values from 0.1 to 1.9
- point_weight: bfloat16 [2048, 2048], replicated, may hold values from -0.125 to 0.125
- residual_in: bfloat16 [16384, 2048], P(('sp', 'tp')), may hold values from -3 to 3
- first_gain: float32 [2048], replicated, may hold values from 0.1 to 1.9
- second_gain: float32 [2048], replicated, may hold values from 0.1 to 1.9
- routes: int32 [16384, 2], P(('sp', 'tp')), may hold values from 0 to 127, all different within a row; in each aligned block of 128 rows (0 to 127, 128 to 255, ...) at most 4 rows name the same one
- route_score: float32 [16384, 2], P(('sp', 'tp')), may hold values from 0.1 to 1
- expert_gate: bfloat16 [128, 2048, 1024], P(('sp', 'tp')), may hold values from -0.125 to 0.125
- expert_up: bfloat16 [128, 2048, 1024], P(('sp', 'tp')), may hold values from -0.125 to 0.125
- expert_down: bfloat16 [128, 1024, 2048], P(('sp', 'tp')), may hold values from -0.1875 to 0.1875
Outputs:
- layer_out: bfloat16 [16384, 2048], P(('sp', 'tp'))
The draws below stay inside these ranges and needn't reach their ends.
Inputs may be any that keep to these rules, and one draw needn't show every extreme that they name: `routes`: among the 128 rows of one device (aligned blocks of rows), no expert is named more than 4 times, a bound that some block reaches; a row names 2 different experts. conv_taps have independent entries, with scales that differ from channel to channel.
All inputs are finite; a program needn't handle non-finite values.
Results may differ from the reference program's by a relative error of at most 0.013.
Values may be sent and summed in bfloat16 or wider, within the bound.
A program may use at most 128 MiB of HBM per device.

```python
import math
import jax
import jax.numpy as jnp
import numpy as np
from jax import lax

D = 2048
FF = 1024
KW = 31
TOP = 2
TOKENS = 16384
ROWS = 128
EXPERTS = 128
MOST = 4


def draw_conv_taps(key, part):
    base_key = jax.random.fold_in(key, 11)
    tap_key, scale_key = jax.random.split(base_key)
    position = jnp.arange(D, dtype=jnp.float32) / D
    rising = 4.0 ** position
    taps = jax.random.normal(tap_key, (KW, D), jnp.float32)
    factor = jnp.exp(jax.random.uniform(scale_key, (1, D), jnp.float32, -0.7, 0.7))
    return (taps * factor * rising[None, :] * (0.5 / KW ** 0.5)).astype(jnp.float32)


def level_of(own_key, dims, shards, smallest, largest):
    factor_of = 1.0
    for dim, parts in shards:
        draws = jax.random.uniform(jax.random.fold_in(jax.random.fold_in(own_key, 6), dim), (parts,), jnp.float32, smallest / len(shards), largest / len(shards))
        factor_of = factor_of * jnp.repeat(jnp.exp(draws), dims[dim] // parts).reshape((-1,) + (1,) * (len(dims) - 1 - dim))
    return factor_of


def routed_block(own_key, own, number, rows, count, top, limit, slope):
    order = jax.random.permutation(own_key, count)
    packed, ordinary = load_shares(count, rows * top, limit, slope, True), load_shares(count, rows * top, limit, slope, False)
    places = jnp.arange(count)

    def named(lengths, offset_by):
        used = int((lengths > 0).sum())
        fixed = max(1, used // 4)
        shifted = fixed + (places - fixed + offset_by * (used - fixed)) % max(1, count - fixed)
        return jnp.zeros((count,), jnp.int32).at[order[jnp.where(places < fixed, places, shifted)]].set(jnp.asarray(lengths, jnp.int32))

    lengths = jnp.where(number % 4 == 0, named(packed, number // 4), named(ordinary, number - number // 4 - 1))
    mixed = jax.random.permutation(jax.random.fold_in(own, 3), count)
    source_of, taker = mixed[0:count // 2 * 2:2], mixed[1:count // 2 * 2:2]
    room = jnp.minimum(lengths[source_of] - 1, limit - lengths[taker]) // 2
    room = jnp.where((source_of == order[0]) | (taker == order[0]) | (lengths[taker] == 0), 0, jnp.maximum(room, 0))
    shifted = jax.random.randint(jax.random.fold_in(own, 4), (count // 2,), 0, 1 << 20) % (room + 1)
    lengths = lengths.at[source_of].add(-shifted).at[taker].add(shifted)
    labels = jnp.searchsorted(jnp.cumsum(lengths), jnp.arange(rows * top), side="right").astype(jnp.int32)
    table = labels.reshape(top, rows).T
    table = table[jax.random.permutation(jax.random.fold_in(own, 1), rows)]
    offset_by = jax.random.randint(jax.random.fold_in(own, 2), (rows, 1), 0, top)
    return jnp.take_along_axis(table, (jnp.arange(top)[None, :] + offset_by) % top, axis=1)


def load_shares(number_of, total, bound, skew, full):
    weights = [(1 << 20) // math.isqrt(standing ** skew) + 1 for standing in range(1, number_of + 1)]
    largest = bound if full else min(bound, max(-(-total // number_of), total * weights[0] // sum(weights)))
    least = 1 if total - largest >= number_of - 1 else 0
    given, rest = [largest] + [least] * (number_of - 1), total - largest - least * (number_of - 1)
    while rest > 0:
        free = [i for i in range(1, number_of) if given[i] < largest] or [i for i in range(1, number_of) if given[i] < bound]
        pool, budget = sum([weights[i] for i in free]), rest
        for i in free:
            more = min(bound - given[i], max(1, budget * weights[i] // pool), rest)
            given[i] = given[i] + more
            rest = rest - more
    return np.array(given)


def gaussian(own_key, shape, deviation, bound, pieces=(), kind=jnp.bfloat16):
    entries = jax.random.normal(own_key, shape, jnp.float32) * deviation
    if len(pieces) > 0:
        entries = level_of(own_key, shape, pieces, -0.22, 0.18) * entries
    return jnp.clip(entries, min=-bound, max=bound).astype(kind)


def setup_inputs(seed: int = 0) -> dict:
    splits = jax.random.split(jax.random.key(seed), 14)
    conv_value = gaussian(splits[0], (TOKENS, D), 1.0, 6.0, ((0, 32), (1, 4)))
    conv_gate = gaussian(splits[1], (TOKENS, D), 1.0, 6.0, ((0, 32), (1, 4)))
    conv_taps = draw_conv_taps(jax.random.fold_in(splits[13], 71), 0)
    channel_gain = jnp.clip(1.0 + 0.18 * jax.random.normal(splits[3], (D,), jnp.float32), 0.1, 1.9)
    point_weight = gaussian(splits[4], (D, D), D ** -0.5, 0.125)
    residual_in = gaussian(splits[5], (TOKENS, D), 0.5, 3.0, ((0, 128),))
    first_gain = jnp.clip(1.0 + 0.18 * jax.random.normal(splits[6], (D,), jnp.float32), 0.1, 1.9)
    second_gain = jnp.clip(1.0 + 0.18 * jax.random.normal(splits[7], (D,), jnp.float32), 0.1, 1.9)
    routes_keys = jax.random.split(jax.random.fold_in(splits[8], 1), TOKENS // ROWS)
    routes_turns = jax.random.permutation(jax.random.fold_in(splits[8], 3), TOKENS // ROWS)
    routes = jax.vmap(lambda own, number: routed_block(jax.random.fold_in(splits[8], 2), own, number, ROWS, EXPERTS, TOP, MOST, 0))(routes_keys, routes_turns).reshape((TOKENS, TOP))
    route_score = jnp.clip(0.1 + 0.9 * jax.random.uniform(splits[9], (TOKENS, TOP), jnp.float32) ** level_of(splits[9], (TOKENS, TOP), ((0, 128),), -0.2, 0.2), 0.1, 1.0)
    expert_gate = gaussian(splits[10], (EXPERTS, D, FF), D ** -0.5, 0.125, ((0, 128),))
    expert_up = gaussian(splits[11], (EXPERTS, D, FF), D ** -0.5, 0.125, ((0, 128),))
    expert_down = gaussian(splits[12], (EXPERTS, FF, D), FF ** -0.5, 0.1875, ((0, 128),))
    return dict(conv_value=conv_value, conv_gate=conv_gate, conv_taps=conv_taps, channel_gain=channel_gain, point_weight=point_weight, residual_in=residual_in, first_gain=first_gain, second_gain=second_gain, routes=routes, route_score=route_score, expert_gate=expert_gate, expert_up=expert_up, expert_down=expert_down)


block_rows = 32
residual_scale = 8.0 ** 0.25

def token_norm(values, gain):
    middle = lax.optimization_barrier(jnp.mean(values, axis=-1, keepdims=True))
    centred = values - middle
    spread = lax.optimization_barrier(jnp.mean(centred * centred, axis=-1, keepdims=True))
    return centred * lax.rsqrt(spread + 1e-05) * gain

def reference(conv_value, conv_gate, conv_taps, channel_gain, point_weight, residual_in, first_gain, second_gain, routes, route_score, expert_gate, expert_up, expert_down):
    glu = conv_value.astype(jnp.float32) * jax.nn.sigmoid(conv_gate.astype(jnp.float32))
    padded_glu = jnp.concatenate([jnp.zeros((KW - 1, D), glu.dtype), glu], axis=0)
    conv = jnp.zeros((TOKENS, D), glu.dtype)
    for tap in range(KW):
        conv = conv + conv_taps[tap][None, :].astype(glu.dtype) * padded_glu[tap:tap + TOKENS]
    middle = lax.optimization_barrier(jnp.mean(conv, axis=1, keepdims=True))
    spread = lax.optimization_barrier(jnp.mean(conv * conv, axis=1, keepdims=True)) - middle * middle
    normed = (conv - middle) * lax.rsqrt(spread + 1e-05) * channel_gain
    act = (normed * jax.nn.sigmoid(normed)).astype(jnp.bfloat16)
    mix = jnp.dot(act, point_weight, preferred_element_type=jnp.float32)
    first = token_norm(residual_scale * residual_in.astype(jnp.float32) + mix, first_gain).astype(jnp.bfloat16)
    total = TOKENS * TOP
    flat_e = routes.reshape(-1).astype(jnp.int32)
    flat_t = (jnp.arange(total, dtype=jnp.int32) // TOP).astype(jnp.int32)
    order = jnp.argsort(flat_e, stable=True).astype(jnp.int32)
    sorted_e = flat_e[order]
    sorted_t = flat_t[order]
    counts = lax.optimization_barrier(jnp.sum((flat_e[:, None] == jnp.arange(EXPERTS, dtype=jnp.int32)[None, :]).astype(jnp.int32), axis=0))
    padded = (counts + block_rows - 1) // block_rows * block_rows
    begin = jnp.cumsum(counts) - counts
    pad_end = jnp.cumsum(padded)
    pad_begin = pad_end - padded
    dest = (pad_begin[sorted_e] + jnp.arange(total, dtype=jnp.int32) - begin[sorted_e]).astype(jnp.int32)
    n_rows = (total + block_rows - 1) // block_rows * block_rows + EXPERTS * block_rows
    n_blocks = n_rows // block_rows
    row_tok = jnp.full((n_rows,), TOKENS, jnp.int32).at[dest].set(sorted_t)
    block_expert = jnp.minimum(jnp.searchsorted(pad_end, jnp.arange(n_blocks, dtype=jnp.int32) * block_rows, side='right'), EXPERTS - 1).astype(jnp.int32)
    padded_first = jnp.concatenate([first, jnp.zeros((1, D), jnp.bfloat16)], axis=0)

    def run_block(inputs):
        tokens_idx, expert = inputs
        rows_in = padded_first[tokens_idx]
        gate = jnp.dot(rows_in, expert_gate[expert], preferred_element_type=jnp.float32)
        upper = jnp.dot(rows_in, expert_up[expert], preferred_element_type=jnp.float32)
        hidden = (jax.nn.silu(gate) * upper).astype(jnp.bfloat16)
        return jnp.dot(hidden, expert_down[expert], preferred_element_type=jnp.float32).astype(jnp.bfloat16)
    answers = lax.map(run_block, (row_tok.reshape(n_blocks, block_rows), block_expert)).reshape(n_rows, D)
    per_assign = jnp.zeros((total, D), jnp.bfloat16).at[order].set(answers[dest])
    share = route_score / lax.optimization_barrier(jnp.sum(route_score, axis=1, keepdims=True))
    moe = lax.optimization_barrier(jnp.sum(share[:, :, None] * per_assign.reshape(TOKENS, TOP, D).astype(jnp.float32), axis=1))
    return token_norm(residual_scale * first.astype(jnp.float32) + moe, second_gain).astype(jnp.bfloat16)
```

```python
import functools

import jax
import jax.numpy as jnp
from jax import lax
from jax.experimental import pallas as pl
from jax.experimental.pallas import tpu as pltpu
from jax.sharding import PartitionSpec as P

residual_scale = 8.0**0.25
MESH = pl.DeviceIdType.MESH
f32, bf16 = jnp.float32, jnp.bfloat16

PEERS, SLOTS, QUARTERS = 128, 4, 4
BLOCK = SLOTS * QUARTERS
HALF = PEERS // 2


def from_behind(block, axis, distance):
    devices = range(lax.axis_size(axis))
    route = [(i - distance, i) for i in devices if i - distance in devices]
    return lax.ppermute(block, axis, route)


def token_norm(values, gain):
    middle = jnp.mean(values, axis=-1, keepdims=True)
    centred = values - middle
    spread = jnp.mean(centred * centred, axis=-1, keepdims=True)
    return centred * lax.rsqrt(spread + 1e-05) * gain


def place():
    sp, x = lax.axis_index("sp"), lax.axis_index("tp")
    return x, (sp // 2) % 4, sp // 8, sp % 2


def partner(n, sign):
    x, y, z, c = place()
    dx, dy, dz, dc = n % 4, (n // 4) % 4, (n // 16) % 4, n // 64
    px, py, pz, pc = (x + sign * dx + 4) % 4, (y + sign * dy + 4) % 4, (z + sign * dz + 4) % 4, (c + dc) % 2
    return {"sp": (pz * 4 + py) * 2 + pc, "tp": px}


def offset_of(e):
    x, y, z, c = place()
    ex, ec, ey, ez = e & 3, (e >> 2) & 1, (e >> 3) & 3, e >> 5
    return ((ec - c) & 1) * 64 + ((ez - z) & 3) * 16 + ((ey - y) & 3) * 4 + ((ex - x) & 3)


def slot_rows(mine, other, earlier, axis):
    return jnp.sum(((mine == other) & earlier).astype(f32), axis=axis, keepdims=True).astype(jnp.int32)


def moe_kernel(
    first_ref,
    routes_ref,
    routes_t_ref,
    score_ref,
    gain_ref,
    gate_hbm,
    up_hbm,
    down_hbm,
    out_ref,
    gate_w,
    up_w,
    down_w,
    send,
    recv,
    flat,
    hidden,
    answer,
    back_send,
    back_recv,
    pick,
    total,
    w_sem,
    send_sem,
    recv_sem,
    back_send_sem,
    back_recv_sem,
):
    barrier = pltpu.get_barrier_semaphore()

    def greet(k, carry):
        pl.semaphore_signal(barrier, inc=1, device_id=partner(k, 1), device_id_type=MESH)
        return carry

    lax.fori_loop(1, PEERS, greet, 0)
    weights = [
        pltpu.make_async_copy(gate_hbm.at[0], gate_w, w_sem.at[0]),
        pltpu.make_async_copy(up_hbm.at[0], up_w, w_sem.at[1]),
        pltpu.make_async_copy(down_hbm.at[0], down_w, w_sem.at[2]),
    ]
    for copy in weights:
        copy.start()

    rows, width = first_ref.shape
    quarter = width // QUARTERS
    col = [routes_ref[:, k : k + 1] for k in range(2)]
    row = [routes_t_ref[k : k + 1, :] for k in range(2)]
    r_id = lax.broadcasted_iota(jnp.int32, (rows, rows), 0)
    c_id = lax.broadcasted_iota(jnp.int32, (rows, rows), 1)
    every = r_id >= 0
    before_l = [
        slot_rows(row[0], col[0], r_id < c_id, 0),
        slot_rows(row[1], col[0], every, 0) + slot_rows(row[1], col[1], r_id < c_id, 0),
    ]
    before_s = [
        slot_rows(col[0], row[0], c_id < r_id, 1),
        slot_rows(col[1], row[0], every, 1) + slot_rows(col[1], row[1], c_id < r_id, 1),
    ]
    where_l = [offset_of(row[k]) * BLOCK + before_l[k] for k in range(2)]
    where_s = [offset_of(col[k]) * BLOCK + before_s[k] for k in range(2)]

    stacked = jnp.concatenate([first_ref[:, q * quarter : (q + 1) * quarter] for q in range(QUARTERS)], axis=0)
    key_l = [jnp.concatenate([where_l[k] + q * SLOTS for q in range(QUARTERS)], axis=1) for k in range(2)]

    def fill(b, carry):
        ids = lax.broadcasted_iota(jnp.int32, (512, QUARTERS * rows), 0) + b * 512
        chosen = ((ids == key_l[0]) | (ids == key_l[1])).astype(f32).astype(bf16)
        picked = jnp.dot(chosen, stacked, preferred_element_type=f32).astype(bf16)
        send[pl.ds(pl.multiple_of(b * 32, 32), 32)] = picked.reshape(32, BLOCK, quarter)
        return carry

    lax.fori_loop(0, PEERS * BLOCK // 512, fill, 0)
    recv[0] = send[0]
    pl.semaphore_wait(barrier, PEERS - 1)

    def dispatch_to(n, h):
        return pltpu.make_async_remote_copy(
            src_ref=send.at[n],
            dst_ref=recv.at[n],
            send_sem=send_sem,
            recv_sem=recv_sem.at[h],
            device_id=partner(n, 1),
            device_id_type=MESH,
        )

    def answer_to(n, h):
        return pltpu.make_async_remote_copy(
            src_ref=back_send.at[n],
            dst_ref=back_recv.at[n],
            send_sem=back_send_sem,
            recv_sem=back_recv_sem.at[h],
            device_id=partner(n, -1),
            device_id_type=MESH,
        )

    def near(k, carry):
        dispatch_to((k * 37) % HALF, 0).start()
        return carry

    def far(k, carry):
        dispatch_to(HALF + (k * 37) % HALF, 1).start()
        return carry

    lax.fori_loop(1, HALF, near, 0)
    lax.fori_loop(0, HALF, far, 0)

    i = lax.broadcasted_iota(jnp.int32, (256, 256), 0)
    j = lax.broadcasted_iota(jnp.int32, (256, 256), 1)
    to_flat = (((i // 4) % 16) * 16 + (i // 64) * 4 + i % 4 == j).astype(f32).astype(bf16)
    to_block = (((j // 4) % 16) * 16 + (j // 64) * 4 + j % 4 == i).astype(f32).astype(bf16)

    for h in range(2):
        start = h * HALF
        own = 1 - h
        landed = recv.at[pl.ds(start + own, HALF - own)]
        pltpu.make_async_copy(landed, landed, recv_sem.at[h]).wait()
        for g in range(4):
            block = recv[pl.ds(start + g * 16, 16)].reshape(256, quarter)
            moved = jnp.dot(to_flat, block, preferred_element_type=f32).astype(bf16)
            for q in range(QUARTERS):
                flat[pl.ds(g * 64, 64), pl.ds(q * quarter, quarter)] = moved[q * 64 : (q + 1) * 64]
        if h == 0:
            for copy in weights:
                copy.wait()

        def hide(b, carry):
            cols = pl.ds(pl.multiple_of(b * 256, 256), 256)
            gate = jnp.dot(flat[...], gate_w[:, cols], preferred_element_type=f32)
            upper = jnp.dot(flat[...], up_w[:, cols], preferred_element_type=f32)
            hidden[:, cols] = (gate * jax.nn.sigmoid(gate) * upper).astype(bf16)
            return carry

        lax.fori_loop(0, hidden.shape[1] // 256, hide, 0)
        for q in range(QUARTERS):
            cols = pl.ds(q * quarter, quarter)
            result = jnp.dot(hidden[...], down_w[:, cols], preferred_element_type=f32).astype(bf16)
            for g in range(4):
                answer[g, pl.ds(q * 64, 64), :] = result[g * 64 : (g + 1) * 64]
        for g in range(4):
            moved = jnp.dot(to_block, answer[g], preferred_element_type=f32).astype(bf16)
            back_send[pl.ds(start + g * 16, 16)] = moved.reshape(16, BLOCK, quarter)
        if h == 0:
            back_recv[0] = back_send[0]

            def near_back(k, carry):
                answer_to((k * 37) % HALF, 0).start()
                return carry

            lax.fori_loop(1, HALF, near_back, 0)
        else:

            def far_back(k, carry):
                answer_to(HALF + (k * 37) % HALF, 1).start()
                return carry

            lax.fori_loop(0, HALF, far_back, 0)

    def choose(b, carry):
        ids = lax.broadcasted_iota(jnp.int32, (rows, PEERS * BLOCK), 1)
        k, q = b // QUARTERS, b % QUARTERS
        key = jnp.where(k == 0, where_s[0], where_s[1]) + q * SLOTS
        pick[pl.ds(pl.multiple_of(b * rows, rows), rows)] = (ids == key).astype(f32).astype(bf16)
        return carry

    lax.fori_loop(0, 2 * QUARTERS, choose, 0)

    for h in range(2):
        start = h * HALF
        own = 1 - h
        landed = back_recv.at[pl.ds(start + own, HALF - own)]
        pltpu.make_async_copy(landed, landed, back_recv_sem.at[h]).wait()
        block = back_recv[pl.ds(start, HALF)].reshape(HALF * BLOCK, quarter)
        part = jnp.dot(
            pick[:, pl.ds(start * BLOCK, HALF * BLOCK)], block, preferred_element_type=f32
        )
        total[...] = part if h == 0 else total[...] + part

    score = score_ref[...]
    share = score / (score[:, 0:1] + score[:, 1:2])
    mixed = []
    for q in range(QUARTERS):
        base = residual_scale * first_ref[:, q * quarter : (q + 1) * quarter].astype(f32)
        one = total[pl.ds(q * rows, rows), :] * share[:, 0:1]
        two = total[pl.ds((QUARTERS + q) * rows, rows), :] * share[:, 1:2]
        mixed.append(base + (one + two))
    middle = sum(jnp.sum(m, axis=1, keepdims=True) for m in mixed) / width
    mixed = [m - middle for m in mixed]
    spread = sum(jnp.sum(m * m, axis=1, keepdims=True) for m in mixed) / width
    scale = lax.rsqrt(spread + 1e-05)
    for q in range(QUARTERS):
        cols = slice(q * quarter, (q + 1) * quarter)
        out_ref[:, cols] = (mixed[q] * scale * gain_ref[:, cols]).astype(bf16)

    sent = send.at[pl.ds(1, PEERS - 1)]
    pltpu.make_async_copy(sent, sent, send_sem).wait()
    sent = back_send.at[pl.ds(1, PEERS - 1)]
    pltpu.make_async_copy(sent, sent, back_send_sem).wait()


def experts_layer(first, routes, score, gain, expert_gate, expert_up, expert_down):
    rows, width = first.shape
    inner = expert_gate.shape[2]
    quarter = width // QUARTERS
    vmem = pl.BlockSpec(memory_space=pltpu.VMEM)
    hbm = pl.BlockSpec(memory_space=pl.ANY)
    blocks = pltpu.VMEM((PEERS, BLOCK, quarter), bf16)
    return pl.pallas_call(
        moe_kernel,
        out_shape=jax.ShapeDtypeStruct((rows, width), bf16),
        in_specs=[vmem] * 5 + [hbm] * 3,
        out_specs=vmem,
        scratch_shapes=[
            pltpu.VMEM((width, inner), bf16),
            pltpu.VMEM((width, inner), bf16),
            pltpu.VMEM((inner, width), bf16),
            blocks,
            blocks,
            pltpu.VMEM((HALF * SLOTS, width), bf16),
            pltpu.VMEM((HALF * SLOTS, inner), bf16),
            pltpu.VMEM((4, 256, quarter), bf16),
            blocks,
            blocks,
            pltpu.VMEM((2 * QUARTERS * rows, PEERS * BLOCK), bf16),
            pltpu.VMEM((2 * QUARTERS * rows, quarter), f32),
            pltpu.SemaphoreType.DMA((3,)),
            pltpu.SemaphoreType.DMA,
            pltpu.SemaphoreType.DMA((2,)),
            pltpu.SemaphoreType.DMA,
            pltpu.SemaphoreType.DMA((2,)),
        ],
        compiler_params=pltpu.CompilerParams(
            collective_id=1, has_side_effects=True, vmem_limit_bytes=56 * 1024 * 1024
        ),
        name="experts",
    )(first, routes, routes.T, score, gain.reshape(1, -1), expert_gate, expert_up, expert_down)


def per_device(
    conv_value,
    conv_gate,
    conv_taps,
    channel_gain,
    point_weight,
    residual_in,
    first_gain,
    second_gain,
    routes,
    route_score,
    expert_gate,
    expert_up,
    expert_down,
):
    edge = conv_taps.shape[0] - 1
    local_width = conv_value.shape[1]
    rim_value, rim_gate = from_behind((conv_value[-edge:], conv_gate[-edge:]), "sp", 1)
    ext_value = jnp.concatenate([rim_value, conv_value], axis=0)
    ext_gate = jnp.concatenate([rim_gate, conv_gate], axis=0)
    glu = ext_value.astype(jnp.float32) * jax.nn.sigmoid(ext_gate.astype(jnp.float32))
    conv = lax.conv_general_dilated(
        glu[None],
        conv_taps[:, None, :],
        (1,),
        [(0, 0)],
        dimension_numbers=("NWC", "WIO", "NWC"),
        feature_group_count=local_width,
    )[0]
    width = local_width * lax.axis_size("tp")
    sums, squares = lax.psum((jnp.sum(conv, axis=1), jnp.sum(conv * conv, axis=1)), "tp")
    middle = sums / width
    spread = squares / width - middle * middle
    normed = (conv - middle[:, None]) * lax.rsqrt(spread + 1e-05)[:, None] * channel_gain
    act = (normed * jax.nn.sigmoid(normed)).astype(jnp.bfloat16)
    owned = lax.all_to_all(act, "tp", split_axis=0, concat_axis=1, tiled=True)
    mix = jnp.dot(owned, point_weight, preferred_element_type=jnp.float32)
    first = token_norm(residual_scale * residual_in.astype(jnp.float32) + mix, first_gain).astype(
        jnp.bfloat16
    )
    return experts_layer(first, routes, route_score, second_gain, expert_gate, expert_up, expert_down)


def solution(mesh):
    in_specs = (
        P("sp", "tp"),
        P("sp", "tp"),
        P(None, "tp"),
        P("tp"),
        P(),
        P(("sp", "tp"), None),
        P(),
        P(),
        P(("sp", "tp"), None),
        P(("sp", "tp"), None),
        P(("sp", "tp"), None, None),
        P(("sp", "tp"), None, None),
        P(("sp", "tp"), None, None),
    )
    out_specs = P(("sp", "tp"), None)
    return jax.shard_map(
        per_device, mesh=mesh, in_specs=in_specs, out_specs=out_specs, check_vma=False
    )
```

```python
import functools

import jax
import jax.numpy as jnp
from jax import lax
from jax.experimental import pallas as pl
from jax.experimental.pallas import tpu as pltpu
from jax.sharding import PartitionSpec as P

residual_scale = 8.0**0.25
MESH = pl.DeviceIdType.MESH
f32, bf16 = jnp.float32, jnp.bfloat16

PEERS, SLOTS, QUARTERS = 128, 4, 4
BLOCK = SLOTS * QUARTERS
HALF = PEERS // 2


def place():
    sp, x = lax.axis_index("sp"), lax.axis_index("tp")
    return x, (sp // 2) % 4, sp // 8, sp % 2


def partner(n, sign):
    x, y, z, c = place()
    dx, dy, dz, dc = n % 4, (n // 4) % 4, (n // 16) % 4, n // 64
    px, py, pz, pc = (x + sign * dx + 4) % 4, (y + sign * dy + 4) % 4, (z + sign * dz + 4) % 4, (c + dc) % 2
    return {"sp": (pz * 4 + py) * 2 + pc, "tp": px}


def offset_of(e):
    x, y, z, c = place()
    ex, ec, ey, ez = e & 3, (e >> 2) & 1, (e >> 3) & 3, e >> 5
    return ((ec - c) & 1) * 64 + ((ez - z) & 3) * 16 + ((ey - y) & 3) * 4 + ((ex - x) & 3)


def slot_rows(mine, other, earlier, axis):
    return jnp.sum(((mine == other) & earlier).astype(f32), axis=axis, keepdims=True).astype(jnp.int32)


def silu(values):
    return values * (1.0 / (1.0 + jnp.exp(-values)))


def across(row):
    n = row.shape[1]
    same = lax.broadcasted_iota(jnp.int32, (n, n), 0) == lax.broadcasted_iota(jnp.int32, (n, n), 1)
    return jnp.sum(jnp.where(same, row, jnp.zeros_like(row)), axis=1, keepdims=True)


def order_of_blocks():
    x = lax.axis_index("tp")
    table = ((2, 1, 3, 0), (3, 2, 0, 1), (3, 1, 0, 2), (1, 2, 0, 3))
    return [
        jnp.where(x == 0, table[0][k], jnp.where(x == 1, table[1][k], jnp.where(x == 2, table[2][k], table[3][k])))
        for k in range(4)
    ]


def layer_kernel(
    value_hbm,
    gate_in_hbm,
    taps_ref,
    channel_gain_ref,
    point_hbm,
    residual_hbm,
    first_gain_ref,
    routes_ref,
    score_ref,
    gate_hbm,
    up_hbm,
    down_hbm,
    out_ref,
    value,
    gate_in,
    rim,
    glu,
    conv_send,
    conv_own,
    conv_recv,
    gains,
    point,
    residual,
    act,
    h1,
    stacked,
    gate_w,
    up_w,
    down_w,
    send,
    recv,
    flat,
    hidden,
    answer,
    back_send,
    back_recv,
    pick,
    total,
    in_sem,
    w_sem,
    rim_sem,
    gain_sem,
    conv_sem,
    send_sem,
    recv_sem,
    back_send_sem,
    back_recv_sem,
):
    inputs = [
        pltpu.make_async_copy(value_hbm, value, in_sem.at[0]),
        pltpu.make_async_copy(gate_in_hbm, gate_in, in_sem.at[1]),
    ]
    weights = [
        pltpu.make_async_copy(point_hbm, point, w_sem.at[0]),
        pltpu.make_async_copy(residual_hbm, residual, w_sem.at[1]),
        pltpu.make_async_copy(gate_hbm.at[0], gate_w, w_sem.at[2]),
        pltpu.make_async_copy(up_hbm.at[0], up_w, w_sem.at[3]),
        pltpu.make_async_copy(down_hbm.at[0], down_w, w_sem.at[4]),
    ]
    for copy in inputs + weights:
        copy.start()
    barrier = pltpu.get_barrier_semaphore()

    def greet(k, carry):
        pl.semaphore_signal(barrier, inc=1, device_id=partner(k, 1), device_id_type=MESH)
        return carry

    lax.fori_loop(1, PEERS, greet, 0)

    rows, quarter = conv_own.shape
    width = quarter * QUARTERS
    taps_n = taps_ref.shape[0]
    lanes = glu.shape[3]
    chunks = quarter // lanes
    lead = glu.shape[2] - rows
    sp, x = lax.axis_index("sp"), lax.axis_index("tp")

    def put_glu(block, values, start):
        for cc in range(chunks):
            glu[block, cc, start : start + values.shape[0], :] = values[:, cc * lanes : (cc + 1) * lanes]

    for copy in inputs:
        copy.wait()
    for p in range(4):
        own = slice(p * rows, (p + 1) * rows)
        gated = value[own, :].astype(f32) * (1.0 / (1.0 + jnp.exp(-gate_in[own, :].astype(f32))))
        put_glu(p, gated, lead)
        if p < 3:
            put_glu(p + 1, gated[rows - lead :], 0)

    def convolve(p, into):
        for cc in range(chunks):
            cols = slice(cc * lanes, (cc + 1) * lanes)
            sum_ = jnp.zeros((rows, lanes), f32)
            for j in range(taps_n):
                sum_ = sum_ + taps_ref[j : j + 1, cols] * glu[p, cc, pl.ds(lead - taps_n + 1 + j, rows), :]
            into[:, cols] = sum_.astype(bf16)

    order = order_of_blocks()
    convolve(order[0], conv_send.at[0])
    pl.semaphore_wait(barrier, PEERS - 1)

    total_rows = value.shape[0]
    behind = {"sp": (sp + 1) % 32, "tp": x}
    rims = [
        pltpu.make_async_remote_copy(
            src_ref=ref.at[pl.ds(total_rows - lead, lead)],
            dst_ref=rim.at[i],
            send_sem=rim_sem.at[0],
            recv_sem=rim_sem.at[1],
            device_id=behind,
            device_id_type=MESH,
        )
        for i, ref in enumerate((value, gate_in))
    ]
    for copy in rims:
        copy.start()

    def conv_to(k):
        return pltpu.make_async_remote_copy(
            src_ref=conv_send.at[k],
            dst_ref=conv_recv.at[(x - order[k] + 4) % 4 - 1],
            send_sem=conv_sem.at[0],
            recv_sem=conv_sem.at[1],
            device_id={"sp": sp, "tp": order[k]},
            device_id_type=MESH,
        )

    def gain_to(d):
        return pltpu.make_async_remote_copy(
            src_ref=channel_gain_ref,
            dst_ref=gains.at[3 - d],
            send_sem=gain_sem.at[0],
            recv_sem=gain_sem.at[1],
            device_id={"sp": sp, "tp": (x + d) % 4},
            device_id_type=MESH,
        )

    conv_to(0).start()
    for d in range(1, 4):
        gain_to(d).start()
    convolve(order[1], conv_send.at[1])
    conv_to(1).start()
    pltpu.make_async_copy(rim, rim, rim_sem.at[1]).wait()
    gated = rim[0].astype(f32) * (1.0 / (1.0 + jnp.exp(-rim[1].astype(f32))))
    put_glu(0, jnp.where(sp > 0, gated, jnp.zeros_like(gated)), 0)
    convolve(order[2], conv_send.at[2])
    conv_to(2).start()
    convolve(order[3], conv_own)

    row = [routes_ref[k : k + 1, :] for k in range(2)]
    col = [across(r) for r in row]
    r_id = lax.broadcasted_iota(jnp.int32, (rows, rows), 0)
    c_id = lax.broadcasted_iota(jnp.int32, (rows, rows), 1)
    every = r_id >= 0
    before_l = [
        slot_rows(row[0], col[0], r_id < c_id, 0),
        slot_rows(row[1], col[0], every, 0) + slot_rows(row[1], col[1], r_id < c_id, 0),
    ]
    before_s = [
        slot_rows(col[0], row[0], c_id < r_id, 1),
        slot_rows(col[1], row[0], every, 1) + slot_rows(col[1], row[1], c_id < r_id, 1),
    ]
    where_l = [offset_of(row[k]) * BLOCK + before_l[k] for k in range(2)]
    where_s = [offset_of(col[k]) * BLOCK + before_s[k] for k in range(2)]
    key_l = [jnp.concatenate([where_l[k] + q * SLOTS for q in range(QUARTERS)], axis=1) for k in range(2)]

    def choose(b, carry):
        ids = lax.broadcasted_iota(jnp.int32, (rows, PEERS * BLOCK), 1)
        k, q = b // QUARTERS, b % QUARTERS
        key = jnp.where(k == 0, where_s[0], where_s[1]) + q * SLOTS
        pick[pl.ds(pl.multiple_of(b * rows, rows), rows)] = (ids == key).astype(f32).astype(bf16)
        return carry

    lax.fori_loop(0, 2 * QUARTERS, choose, 0)

    pltpu.make_async_copy(conv_recv, conv_recv, conv_sem.at[1]).wait()
    pltpu.make_async_copy(gains, gains, gain_sem.at[1]).wait()
    parts = [conv_own[...].astype(f32)] + [conv_recv[i].astype(f32) for i in range(3)]
    middle = sum(jnp.sum(v, axis=1, keepdims=True) for v in parts) / width
    spread = sum(jnp.sum(v * v, axis=1, keepdims=True) for v in parts) / width - middle * middle
    scale = lax.rsqrt(spread + 1e-05)
    for i in range(4):
        gain = channel_gain_ref[...] if i == 0 else gains[i - 1]
        act[i] = silu((parts[i] - middle) * scale * gain).astype(bf16)
    for copy in weights[:2]:
        copy.wait()

    def mix(b, carry):
        cols = pl.ds(pl.multiple_of(b * quarter, quarter), quarter)
        sum_ = residual_scale * residual[:, cols].astype(f32)
        for i in range(4):
            block = (x + i) % 4
            sum_ = sum_ + jnp.dot(
                act[i],
                point[pl.ds(pl.multiple_of(block * quarter, quarter), quarter), cols],
                preferred_element_type=f32,
            )
        h1[b] = sum_
        return carry

    lax.fori_loop(0, QUARTERS, mix, 0)
    middle = sum(jnp.sum(h1[q], axis=1, keepdims=True) for q in range(QUARTERS)) / width
    centred = [h1[q] - middle for q in range(QUARTERS)]
    spread = sum(jnp.sum(v * v, axis=1, keepdims=True) for v in centred) / width
    scale = lax.rsqrt(spread + 1e-05)
    for q in range(QUARTERS):
        cols = slice(q * quarter, (q + 1) * quarter)
        stacked[pl.ds(q * rows, rows), :] = (centred[q] * scale * first_gain_ref[:, cols]).astype(bf16)

    def fill(b, carry):
        ids = lax.broadcasted_iota(jnp.int32, (512, QUARTERS * rows), 0) + b * 512
        chosen = ((ids == key_l[0]) | (ids == key_l[1])).astype(f32).astype(bf16)
        picked = jnp.dot(chosen, stacked[...], preferred_element_type=f32).astype(bf16)
        send[pl.ds(pl.multiple_of(b * 32, 32), 32)] = picked.reshape(32, BLOCK, quarter)
        return carry

    lax.fori_loop(0, PEERS * BLOCK // 512, fill, 0)
    recv[0] = send[0]
    def dispatch_to(n, h):
        return pltpu.make_async_remote_copy(
            src_ref=send.at[n],
            dst_ref=recv.at[n],
            send_sem=send_sem,
            recv_sem=recv_sem.at[h],
            device_id=partner(n, 1),
            device_id_type=MESH,
        )

    def answer_to(n, h):
        return pltpu.make_async_remote_copy(
            src_ref=back_send.at[n],
            dst_ref=back_recv.at[n],
            send_sem=back_send_sem,
            recv_sem=back_recv_sem.at[h],
            device_id=partner(n, -1),
            device_id_type=MESH,
        )

    def near(k, carry):
        dispatch_to((k * 37) % HALF, 0).start()
        return carry

    def far(k, carry):
        dispatch_to(HALF + (k * 37) % HALF, 1).start()
        return carry

    lax.fori_loop(1, HALF, near, 0)
    lax.fori_loop(0, HALF, far, 0)

    i = lax.broadcasted_iota(jnp.int32, (256, 256), 0)
    j = lax.broadcasted_iota(jnp.int32, (256, 256), 1)
    to_flat = (((i // 4) % 16) * 16 + (i // 64) * 4 + i % 4 == j).astype(f32).astype(bf16)
    to_block = (((j // 4) % 16) * 16 + (j // 64) * 4 + j % 4 == i).astype(f32).astype(bf16)

    for h in range(2):
        start = h * HALF
        own = 1 - h
        landed = recv.at[pl.ds(start + own, HALF - own)]
        pltpu.make_async_copy(landed, landed, recv_sem.at[h]).wait()
        for g in range(4):
            block = recv[pl.ds(start + g * 16, 16)].reshape(256, quarter)
            moved = jnp.dot(to_flat, block, preferred_element_type=f32).astype(bf16)
            for q in range(QUARTERS):
                flat[pl.ds(g * 64, 64), pl.ds(q * quarter, quarter)] = moved[q * 64 : (q + 1) * 64]
        if h == 0:
            for copy in weights[2:]:
                copy.wait()

        def hide(b, carry):
            cols = pl.ds(pl.multiple_of(b * 256, 256), 256)
            gate = jnp.dot(flat[...], gate_w[:, cols], preferred_element_type=f32)
            upper = jnp.dot(flat[...], up_w[:, cols], preferred_element_type=f32)
            hidden[:, cols] = (gate * jax.nn.sigmoid(gate) * upper).astype(bf16)
            return carry

        lax.fori_loop(0, hidden.shape[1] // 256, hide, 0)
        for q in range(QUARTERS):
            cols = pl.ds(q * quarter, quarter)
            result = jnp.dot(hidden[...], down_w[:, cols], preferred_element_type=f32).astype(bf16)
            for g in range(4):
                answer[g, pl.ds(q * 64, 64), :] = result[g * 64 : (g + 1) * 64]
        for g in range(4):
            moved = jnp.dot(to_block, answer[g], preferred_element_type=f32).astype(bf16)
            back_send[pl.ds(start + g * 16, 16)] = moved.reshape(16, BLOCK, quarter)
        if h == 0:
            back_recv[0] = back_send[0]

            def near_back(k, carry):
                answer_to((k * 37) % HALF, 0).start()
                return carry

            lax.fori_loop(1, HALF, near_back, 0)
        else:

            def far_back(k, carry):
                answer_to(HALF + (k * 37) % HALF, 1).start()
                return carry

            lax.fori_loop(0, HALF, far_back, 0)

    for h in range(2):
        start = h * HALF
        own = 1 - h
        landed = back_recv.at[pl.ds(start + own, HALF - own)]
        pltpu.make_async_copy(landed, landed, back_recv_sem.at[h]).wait()
        block = back_recv[pl.ds(start, HALF)].reshape(HALF * BLOCK, quarter)
        part = jnp.dot(
            pick[:, pl.ds(start * BLOCK, HALF * BLOCK)], block, preferred_element_type=f32
        )
        total[...] = part if h == 0 else total[...] + part

    share = [across(score_ref[k : k + 1, :] / (score_ref[0:1, :] + score_ref[1:2, :])) for k in range(2)]
    mixed = []
    for q in range(QUARTERS):
        base = residual_scale * stacked[pl.ds(q * rows, rows), :].astype(f32)
        one = total[pl.ds(q * rows, rows), :] * share[0]
        two = total[pl.ds((QUARTERS + q) * rows, rows), :] * share[1]
        mixed.append(base + (one + two))
    middle = sum(jnp.sum(m, axis=1, keepdims=True) for m in mixed) / width
    mixed = [m - middle for m in mixed]
    spread = sum(jnp.sum(m * m, axis=1, keepdims=True) for m in mixed) / width
    scale = lax.rsqrt(spread + 1e-05)
    for q in range(QUARTERS):
        out_ref[:, q * quarter : (q + 1) * quarter] = mixed[q] * scale

    for copy in rims:
        copy.wait_send()
    for k in range(3):
        conv_to(k).wait_send()
    for d in range(1, 4):
        gain_to(d).wait_send()
    sent = send.at[pl.ds(1, PEERS - 1)]
    pltpu.make_async_copy(sent, sent, send_sem).wait()
    sent = back_send.at[pl.ds(1, PEERS - 1)]
    pltpu.make_async_copy(sent, sent, back_send_sem).wait()


def per_device(
    conv_value,
    conv_gate,
    conv_taps,
    channel_gain,
    point_weight,
    residual_in,
    first_gain,
    second_gain,
    routes,
    route_score,
    expert_gate,
    expert_up,
    expert_down,
):
    rows, width = residual_in.shape
    inner = expert_gate.shape[2]
    tokens, quarter = conv_value.shape
    lanes = 128
    lead = -(-(conv_taps.shape[0] - 1) // 16) * 16
    vmem = pl.BlockSpec(memory_space=pltpu.VMEM)
    hbm = pl.BlockSpec(memory_space=pl.ANY)
    blocks = pltpu.VMEM((PEERS, BLOCK, quarter), bf16)
    dma = pltpu.SemaphoreType.DMA
    normed = pl.pallas_call(
        layer_kernel,
        out_shape=jax.ShapeDtypeStruct((rows, width), f32),
        in_specs=[hbm, hbm, vmem, vmem, hbm, hbm, vmem, vmem, vmem, hbm, hbm, hbm],
        out_specs=vmem,
        scratch_shapes=[
            pltpu.VMEM((tokens, quarter), bf16),
            pltpu.VMEM((tokens, quarter), bf16),
            pltpu.VMEM((2, lead, quarter), bf16),
            pltpu.VMEM((4, quarter // lanes, lead + rows, lanes), f32),
            pltpu.VMEM((3, rows, quarter), bf16),
            pltpu.VMEM((rows, quarter), bf16),
            pltpu.VMEM((3, rows, quarter), bf16),
            pltpu.VMEM((3, 1, quarter), f32),
            pltpu.VMEM((width, width), bf16),
            pltpu.VMEM((rows, width), bf16),
            pltpu.VMEM((4, rows, quarter), bf16),
            pltpu.VMEM((QUARTERS, rows, quarter), f32),
            pltpu.VMEM((QUARTERS * rows, quarter), bf16),
            pltpu.VMEM((width, inner), bf16),
            pltpu.VMEM((width, inner), bf16),
            pltpu.VMEM((inner, width), bf16),
            blocks,
            blocks,
            pltpu.VMEM((HALF * SLOTS, width), bf16),
            pltpu.VMEM((HALF * SLOTS, inner), bf16),
            pltpu.VMEM((4, 256, quarter), bf16),
            blocks,
            blocks,
            pltpu.VMEM((2 * QUARTERS * rows, PEERS * BLOCK), bf16),
            pltpu.VMEM((2 * QUARTERS * rows, quarter), f32),
            dma((2,)),
            dma((5,)),
            dma((2,)),
            dma((2,)),
            dma((2,)),
            dma,
            dma((2,)),
            dma,
            dma((2,)),
        ],
        compiler_params=pltpu.CompilerParams(
            collective_id=1, has_side_effects=True, vmem_limit_bytes=60 * 1024 * 1024
        ),
        name="layer",
    )(
        conv_value,
        conv_gate,
        conv_taps,
        channel_gain.reshape(1, -1),
        point_weight,
        residual_in,
        first_gain.reshape(1, -1),
        routes.T,
        route_score.T,
        expert_gate,
        expert_up,
        expert_down,
    )
    return (normed * second_gain).astype(bf16)


def solution(mesh):
    in_specs = (
        P("sp", "tp"),
        P("sp", "tp"),
        P(None, "tp"),
        P("tp"),
        P(),
        P(("sp", "tp"), None),
        P(),
        P(),
        P(("sp", "tp"), None),
        P(("sp", "tp"), None),
        P(("sp", "tp"), None, None),
        P(("sp", "tp"), None, None),
        P(("sp", "tp"), None, None),
    )
    out_specs = P(("sp", "tp"), None)
    return jax.shard_map(
        per_device, mesh=mesh, in_specs=in_specs, out_specs=out_specs, check_vma=False
    )
```

```python
import functools

import jax
import jax.numpy as jnp
from jax import lax
from jax.experimental import pallas as pl
from jax.experimental.pallas import tpu as pltpu
from jax.sharding import PartitionSpec as P

residual_scale = 8.0**0.25
MESH = pl.DeviceIdType.MESH
f32, bf16 = jnp.float32, jnp.bfloat16

PEERS, SLOTS, QUARTERS = 128, 4, 4
BLOCK = SLOTS * QUARTERS
HALF = PEERS // 2


def place():
    sp, x = lax.axis_index("sp"), lax.axis_index("tp")
    return x, (sp // 2) % 4, sp // 8, sp % 2


def partner(n, sign):
    x, y, z, c = place()
    dx, dy, dz, dc = n % 4, (n // 4) % 4, (n // 16) % 4, n // 64
    px, py, pz, pc = (x + sign * dx + 4) % 4, (y + sign * dy + 4) % 4, (z + sign * dz + 4) % 4, (c + dc) % 2
    return {"sp": (pz * 4 + py) * 2 + pc, "tp": px}


def offset_of(e):
    x, y, z, c = place()
    ex, ec, ey, ez = e & 3, (e >> 2) & 1, (e >> 3) & 3, e >> 5
    return ((ec - c) & 1) * 64 + ((ez - z) & 3) * 16 + ((ey - y) & 3) * 4 + ((ex - x) & 3)


def slot_rows(mine, other, earlier, axis):
    return jnp.sum(((mine == other) & earlier).astype(f32), axis=axis, keepdims=True).astype(jnp.int32)


def silu(values):
    return values * (1.0 / (1.0 + jnp.exp(-values)))


def across(row):
    n = row.shape[1]
    same = lax.broadcasted_iota(jnp.int32, (n, n), 0) == lax.broadcasted_iota(jnp.int32, (n, n), 1)
    return jnp.sum(jnp.where(same, row, jnp.zeros_like(row)), axis=1, keepdims=True)


def order_of_blocks():
    x = lax.axis_index("tp")
    table = ((2, 1, 3, 0), (3, 2, 0, 1), (3, 1, 0, 2), (1, 2, 0, 3))
    return [
        jnp.where(x == 0, table[0][k], jnp.where(x == 1, table[1][k], jnp.where(x == 2, table[2][k], table[3][k])))
        for k in range(4)
    ]


def layer_kernel(
    value_hbm,
    gate_in_hbm,
    taps_ref,
    channel_gain_ref,
    point_hbm,
    residual_hbm,
    first_gain_ref,
    routes_ref,
    score_ref,
    gate_hbm,
    up_hbm,
    down_hbm,
    out_ref,
    value,
    gate_in,
    rim,
    glu,
    conv_send,
    conv_own,
    conv_recv,
    gains,
    point,
    residual,
    act,
    h1,
    stacked,
    gate_w,
    up_w,
    down_w,
    send,
    recv,
    flat,
    hidden,
    answer,
    back_send,
    back_recv,
    pick,
    total,
    in_sem,
    w_sem,
    rim_sem,
    gain_sem,
    conv_sem,
    send_sem,
    recv_sem,
    back_send_sem,
    back_recv_sem,
    word,
):
    inputs = [
        pltpu.make_async_copy(value_hbm, value, in_sem.at[0]),
        pltpu.make_async_copy(gate_in_hbm, gate_in, in_sem.at[1]),
    ]
    weights = [
        pltpu.make_async_copy(point_hbm, point, w_sem.at[0]),
        pltpu.make_async_copy(residual_hbm, residual, w_sem.at[1]),
        pltpu.make_async_copy(gate_hbm.at[0], gate_w, w_sem.at[2]),
        pltpu.make_async_copy(up_hbm.at[0], up_w, w_sem.at[3]),
        pltpu.make_async_copy(down_hbm.at[0], down_w, w_sem.at[4]),
    ]
    for copy in inputs:
        copy.start()
    barrier = pltpu.get_barrier_semaphore()

    sp, x = lax.axis_index("sp"), lax.axis_index("tp")
    x_line = [partner(d, 1) for d in (1, 2, 3)]
    y_line = [partner(4 * d, 1) for d in (1, 2, 3)]
    z_line = [partner(16 * d, 1) for d in (1, 2, 3)]
    twin = partner(HALF, 1)
    beside = {"sp": (sp + 2 * (sp % 2) - 1 + 32) % 32, "tp": x}
    met = x_line + y_line + z_line + [twin, beside]
    for device in met:
        pl.semaphore_signal(barrier, inc=1, device_id=device, device_id_type=MESH)

    def spread_word(i, line):
        for device in line:
            pl.semaphore_signal(word.at[i], inc=1, device_id=device, device_id_type=MESH)

    rows, quarter = conv_own.shape
    width = quarter * QUARTERS
    taps_n = taps_ref.shape[0]
    lanes = glu.shape[3]
    chunks = quarter // lanes
    lead = glu.shape[2] - rows

    def put_glu(block, values, start):
        for cc in range(chunks):
            glu[block, cc, start : start + values.shape[0], :] = values[:, cc * lanes : (cc + 1) * lanes]

    for copy in inputs:
        copy.wait()
    for copy in weights:
        copy.start()
    for p in range(4):
        own = slice(p * rows, (p + 1) * rows)
        gated = value[own, :].astype(f32) * (1.0 / (1.0 + jnp.exp(-gate_in[own, :].astype(f32))))
        put_glu(p, gated, lead)
        if p < 3:
            put_glu(p + 1, gated[rows - lead :], 0)

    def convolve(p, into, first_row=0, end=rows):
        for cc in range(chunks):
            cols = slice(cc * lanes, (cc + 1) * lanes)
            sum_ = jnp.zeros((end - first_row, lanes), f32)
            for j in range(taps_n):
                start = first_row + lead - taps_n + 1 + j
                sum_ = sum_ + taps_ref[j : j + 1, cols] * glu[p, cc, pl.ds(start, end - first_row), :]
            into[first_row:end, cols] = sum_.astype(bf16)

    order = order_of_blocks()

    def conv_to(k, first_row=0, end=rows):
        return pltpu.make_async_remote_copy(
            src_ref=conv_send.at[k, pl.ds(first_row, end - first_row)],
            dst_ref=conv_recv.at[(x - order[k] + 4) % 4 - 1, pl.ds(first_row, end - first_row)],
            send_sem=conv_sem.at[0],
            recv_sem=conv_sem.at[1],
            device_id={"sp": sp, "tp": order[k]},
            device_id_type=MESH,
        )

    def gain_to(d):
        return pltpu.make_async_remote_copy(
            src_ref=channel_gain_ref,
            dst_ref=gains.at[3 - d],
            send_sem=gain_sem.at[0],
            recv_sem=gain_sem.at[1],
            device_id={"sp": sp, "tp": (x + d) % 4},
            device_id_type=MESH,
        )

    total_rows = value.shape[0]
    behind = {"sp": (sp + 1) % 32, "tp": x}
    rims = [
        pltpu.make_async_remote_copy(
            src_ref=ref.at[pl.ds(total_rows - lead, lead)],
            dst_ref=rim.at[i],
            send_sem=rim_sem.at[0],
            recv_sem=rim_sem.at[1],
            device_id=behind,
            device_id_type=MESH,
        )
        for i, ref in enumerate((value, gate_in))
    ]
    convolve(order[0], conv_send.at[0])
    pl.semaphore_wait(barrier, len(met))
    for copy in rims:
        copy.start()
    conv_to(0).start()
    convolve(order[1], conv_send.at[1])
    conv_to(1).start()
    convolve(order[2], conv_send.at[2], lead, rows)
    conv_to(2, lead, rows).start()
    for d in range(1, 4):
        gain_to(d).start()
    spread_word(0, y_line)
    pltpu.make_async_copy(rim, rim, rim_sem.at[1]).wait()
    gated = rim[0].astype(f32) * (1.0 / (1.0 + jnp.exp(-rim[1].astype(f32))))
    put_glu(0, jnp.where(sp > 0, gated, jnp.zeros_like(gated)), 0)
    convolve(order[2], conv_send.at[2], 0, lead)
    conv_to(2, 0, lead).start()
    pl.semaphore_wait(word.at[0], 3)
    spread_word(1, z_line)
    convolve(order[3], conv_own)

    row = [routes_ref[k : k + 1, :] for k in range(2)]
    col = [across(r) for r in row]
    r_id = lax.broadcasted_iota(jnp.int32, (rows, rows), 0)
    c_id = lax.broadcasted_iota(jnp.int32, (rows, rows), 1)
    every = r_id >= 0
    before_l = [
        slot_rows(row[0], col[0], r_id < c_id, 0),
        slot_rows(row[1], col[0], every, 0) + slot_rows(row[1], col[1], r_id < c_id, 0),
    ]
    before_s = [
        slot_rows(col[0], row[0], c_id < r_id, 1),
        slot_rows(col[1], row[0], every, 1) + slot_rows(col[1], row[1], c_id < r_id, 1),
    ]
    where_l = [offset_of(row[k]) * BLOCK + before_l[k] for k in range(2)]
    where_s = [offset_of(col[k]) * BLOCK + before_s[k] for k in range(2)]
    key_l = [jnp.concatenate([where_l[k] + q * SLOTS for q in range(QUARTERS)], axis=1) for k in range(2)]

    def choose(b, carry):
        ids = lax.broadcasted_iota(jnp.int32, (rows, PEERS * BLOCK), 1)
        k, q = b // QUARTERS, b % QUARTERS
        key = jnp.where(k == 0, where_s[0], where_s[1]) + q * SLOTS
        pick[pl.ds(pl.multiple_of(b * rows, rows), rows)] = (ids == key).astype(f32).astype(bf16)
        return carry

    lax.fori_loop(0, QUARTERS, choose, 0)
    pl.semaphore_wait(word.at[1], 3)
    spread_word(2, [twin])
    lax.fori_loop(QUARTERS, 2 * QUARTERS, choose, 0)

    pltpu.make_async_copy(conv_recv, conv_recv, conv_sem.at[1]).wait()
    pltpu.make_async_copy(gains, gains, gain_sem.at[1]).wait()
    parts = [conv_own[...].astype(f32)] + [conv_recv[i].astype(f32) for i in range(3)]
    middle = sum(jnp.sum(v, axis=1, keepdims=True) for v in parts) / width
    spread = sum(jnp.sum(v * v, axis=1, keepdims=True) for v in parts) / width - middle * middle
    scale = lax.rsqrt(spread + 1e-05)
    for i in range(4):
        gain = channel_gain_ref[...] if i == 0 else gains[i - 1]
        act[i] = silu((parts[i] - middle) * scale * gain).astype(bf16)
    for copy in weights[:2]:
        copy.wait()

    def mix(b, carry):
        cols = pl.ds(pl.multiple_of(b * quarter, quarter), quarter)
        sum_ = residual_scale * residual[:, cols].astype(f32)
        for i in range(4):
            block = (x + i) % 4
            sum_ = sum_ + jnp.dot(
                act[i],
                point[pl.ds(pl.multiple_of(block * quarter, quarter), quarter), cols],
                preferred_element_type=f32,
            )
        h1[b] = sum_
        return carry

    lax.fori_loop(0, QUARTERS, mix, 0)
    middle = sum(jnp.sum(h1[q], axis=1, keepdims=True) for q in range(QUARTERS)) / width
    centred = [h1[q] - middle for q in range(QUARTERS)]
    spread = sum(jnp.sum(v * v, axis=1, keepdims=True) for v in centred) / width
    scale = lax.rsqrt(spread + 1e-05)
    for q in range(QUARTERS):
        cols = slice(q * quarter, (q + 1) * quarter)
        stacked[pl.ds(q * rows, rows), :] = (centred[q] * scale * first_gain_ref[:, cols]).astype(bf16)

    def fill(b, carry):
        ids = lax.broadcasted_iota(jnp.int32, (512, QUARTERS * rows), 0) + b * 512
        chosen = ((ids == key_l[0]) | (ids == key_l[1])).astype(f32).astype(bf16)
        picked = jnp.dot(chosen, stacked[...], preferred_element_type=f32).astype(bf16)
        send[pl.ds(pl.multiple_of(b * 32, 32), 32)] = picked.reshape(32, BLOCK, quarter)
        return carry

    pl.semaphore_wait(word.at[2], 1)
    def dispatch_to(n, h):
        return pltpu.make_async_remote_copy(
            src_ref=send.at[n],
            dst_ref=recv.at[n],
            send_sem=send_sem,
            recv_sem=recv_sem.at[h],
            device_id=partner(n, 1),
            device_id_type=MESH,
        )

    def answer_to(n, h):
        return pltpu.make_async_remote_copy(
            src_ref=back_send.at[n],
            dst_ref=back_recv.at[n],
            send_sem=back_send_sem,
            recv_sem=back_recv_sem.at[h],
            device_id=partner(n, -1),
            device_id_type=MESH,
        )

    def near(k, carry):
        dispatch_to((k * 37) % HALF, 0).start()
        return carry

    def far(k, carry):
        dispatch_to(HALF + (k * 37) % HALF, 1).start()
        return carry

    lax.fori_loop(0, HALF * BLOCK // 512, fill, 0)
    lax.fori_loop(1, HALF, near, 0)
    lax.fori_loop(HALF * BLOCK // 512, PEERS * BLOCK // 512, fill, 0)
    lax.fori_loop(0, HALF, far, 0)
    recv[0] = send[0]

    i = lax.broadcasted_iota(jnp.int32, (256, 256), 0)
    j = lax.broadcasted_iota(jnp.int32, (256, 256), 1)
    to_flat = (((i // 4) % 16) * 16 + (i // 64) * 4 + i % 4 == j).astype(f32).astype(bf16)
    to_block = (((j // 4) % 16) * 16 + (j // 64) * 4 + j % 4 == i).astype(f32).astype(bf16)

    for h in range(2):
        start = h * HALF
        own = 1 - h
        landed = recv.at[pl.ds(start + own, HALF - own)]
        pltpu.make_async_copy(landed, landed, recv_sem.at[h]).wait()
        for g in range(4):
            block = recv[pl.ds(start + g * 16, 16)].reshape(256, quarter)
            moved = jnp.dot(to_flat, block, preferred_element_type=f32).astype(bf16)
            for q in range(QUARTERS):
                flat[pl.ds(g * 64, 64), pl.ds(q * quarter, quarter)] = moved[q * 64 : (q + 1) * 64]
        if h == 0:
            for copy in weights[2:]:
                copy.wait()

        def hide(b, carry):
            cols = pl.ds(pl.multiple_of(b * 256, 256), 256)
            gate = jnp.dot(flat[...], gate_w[:, cols], preferred_element_type=f32)
            upper = jnp.dot(flat[...], up_w[:, cols], preferred_element_type=f32)
            hidden[:, cols] = (gate * jax.nn.sigmoid(gate) * upper).astype(bf16)
            return carry

        lax.fori_loop(0, hidden.shape[1] // 256, hide, 0)
        for q in range(QUARTERS):
            cols = pl.ds(q * quarter, quarter)
            result = jnp.dot(hidden[...], down_w[:, cols], preferred_element_type=f32).astype(bf16)
            for g in range(4):
                answer[g, pl.ds(q * 64, 64), :] = result[g * 64 : (g + 1) * 64]
        for g in range(4):
            moved = jnp.dot(to_block, answer[g], preferred_element_type=f32).astype(bf16)
            back_send[pl.ds(start + g * 16, 16)] = moved.reshape(16, BLOCK, quarter)
        if h == 0:
            back_recv[0] = back_send[0]

            def near_back(k, carry):
                answer_to((k * 37) % HALF, 0).start()
                return carry

            lax.fori_loop(1, HALF, near_back, 0)
        else:

            def far_back(k, carry):
                answer_to(HALF + (k * 37) % HALF, 1).start()
                return carry

            lax.fori_loop(0, HALF, far_back, 0)

    for h in range(2):
        start = h * HALF
        own = 1 - h
        landed = back_recv.at[pl.ds(start + own, HALF - own)]
        pltpu.make_async_copy(landed, landed, back_recv_sem.at[h]).wait()
        block = back_recv[pl.ds(start, HALF)].reshape(HALF * BLOCK, quarter)
        part = jnp.dot(
            pick[:, pl.ds(start * BLOCK, HALF * BLOCK)], block, preferred_element_type=f32
        )
        total[...] = part if h == 0 else total[...] + part

    share = [across(score_ref[k : k + 1, :] / (score_ref[0:1, :] + score_ref[1:2, :])) for k in range(2)]
    mixed = []
    for q in range(QUARTERS):
        base = residual_scale * stacked[pl.ds(q * rows, rows), :].astype(f32)
        one = total[pl.ds(q * rows, rows), :] * share[0]
        two = total[pl.ds((QUARTERS + q) * rows, rows), :] * share[1]
        mixed.append(base + (one + two))
    middle = sum(jnp.sum(m, axis=1, keepdims=True) for m in mixed) / width
    mixed = [m - middle for m in mixed]
    spread = sum(jnp.sum(m * m, axis=1, keepdims=True) for m in mixed) / width
    scale = lax.rsqrt(spread + 1e-05)
    for q in range(QUARTERS):
        out_ref[:, q * quarter : (q + 1) * quarter] = mixed[q] * scale

    for copy in rims:
        copy.wait_send()
    for k in range(3):
        conv_to(k).wait_send()
    for d in range(1, 4):
        gain_to(d).wait_send()
    sent = send.at[pl.ds(1, PEERS - 1)]
    pltpu.make_async_copy(sent, sent, send_sem).wait()
    sent = back_send.at[pl.ds(1, PEERS - 1)]
    pltpu.make_async_copy(sent, sent, back_send_sem).wait()


def per_device(
    conv_value,
    conv_gate,
    conv_taps,
    channel_gain,
    point_weight,
    residual_in,
    first_gain,
    second_gain,
    routes,
    route_score,
    expert_gate,
    expert_up,
    expert_down,
):
    rows, width = residual_in.shape
    inner = expert_gate.shape[2]
    tokens, quarter = conv_value.shape
    lanes = 128
    lead = -(-(conv_taps.shape[0] - 1) // 16) * 16
    vmem = pl.BlockSpec(memory_space=pltpu.VMEM)
    hbm = pl.BlockSpec(memory_space=pl.ANY)
    blocks = pltpu.VMEM((PEERS, BLOCK, quarter), bf16)
    dma = pltpu.SemaphoreType.DMA
    normed = pl.pallas_call(
        layer_kernel,
        out_shape=pltpu.VMEM((rows, width), f32),
        in_specs=[hbm, hbm, vmem, vmem, hbm, hbm, vmem, vmem, vmem, hbm, hbm, hbm],
        out_specs=vmem,
        scratch_shapes=[
            pltpu.VMEM((tokens, quarter), bf16),
            pltpu.VMEM((tokens, quarter), bf16),
            pltpu.VMEM((2, lead, quarter), bf16),
            pltpu.VMEM((4, quarter // lanes, lead + rows, lanes), f32),
            pltpu.VMEM((3, rows, quarter), bf16),
            pltpu.VMEM((rows, quarter), bf16),
            pltpu.VMEM((3, rows, quarter), bf16),
            pltpu.VMEM((3, 1, quarter), f32),
            pltpu.VMEM((width, width), bf16),
            pltpu.VMEM((rows, width), bf16),
            pltpu.VMEM((4, rows, quarter), bf16),
            pltpu.VMEM((QUARTERS, rows, quarter), f32),
            pltpu.VMEM((QUARTERS * rows, quarter), bf16),
            pltpu.VMEM((width, inner), bf16),
            pltpu.VMEM((width, inner), bf16),
            pltpu.VMEM((inner, width), bf16),
            blocks,
            blocks,
            pltpu.VMEM((HALF * SLOTS, width), bf16),
            pltpu.VMEM((HALF * SLOTS, inner), bf16),
            pltpu.VMEM((4, 256, quarter), bf16),
            blocks,
            blocks,
            pltpu.VMEM((2 * QUARTERS * rows, PEERS * BLOCK), bf16),
            pltpu.VMEM((2 * QUARTERS * rows, quarter), f32),
            dma((2,)),
            dma((5,)),
            dma((2,)),
            dma((2,)),
            dma((2,)),
            dma,
            dma((2,)),
            dma,
            dma((2,)),
            pltpu.SemaphoreType.REGULAR((3,)),
        ],
        compiler_params=pltpu.CompilerParams(
            collective_id=1, has_side_effects=True, vmem_limit_bytes=60 * 1024 * 1024
        ),
        name="layer",
    )(
        conv_value,
        conv_gate,
        conv_taps,
        channel_gain.reshape(1, -1),
        point_weight,
        residual_in,
        first_gain.reshape(1, -1),
        routes.T,
        route_score.T,
        expert_gate,
        expert_up,
        expert_down,
    )
    return (normed * second_gain).astype(bf16)


def solution(mesh):
    in_specs = (
        P("sp", "tp"),
        P("sp", "tp"),
        P(None, "tp"),
        P("tp"),
        P(),
        P(("sp", "tp"), None),
        P(),
        P(),
        P(("sp", "tp"), None),
        P(("sp", "tp"), None),
        P(("sp", "tp"), None, None),
        P(("sp", "tp"), None, None),
        P(("sp", "tp"), None, None),
    )
    out_specs = P(("sp", "tp"), None)
    return jax.shard_map(
        per_device, mesh=mesh, in_specs=in_specs, out_specs=out_specs, check_vma=False
    )
```

```python
import functools

import jax
import jax.numpy as jnp
from jax import lax
from jax.experimental import pallas as pl
from jax.experimental.pallas import tpu as pltpu
from jax.sharding import PartitionSpec as P

residual_scale = 8.0**0.25
MESH = pl.DeviceIdType.MESH
f32, bf16 = jnp.float32, jnp.bfloat16

PEERS, SLOTS, QUARTERS = 128, 4, 4
BLOCK = SLOTS * QUARTERS
HALF = PEERS // 2
PARTS = ((0, 32), (32, 32), (64, 32), (96, 32))


def far_to_near(part):
    first, count = part
    hops = (0, 1, 2, 1)
    return [n for n in (first + (k * 37) % count for k in range(count)) if n > 0]


def place():
    sp, x = lax.axis_index("sp"), lax.axis_index("tp")
    return x, (sp // 2) % 4, sp // 8, sp % 2


def partner(n, sign):
    x, y, z, c = place()
    dx, dy, dz, dc = n % 4, (n // 4) % 4, (n // 16) % 2 * 2 + (n // 32) % 2, n // 64
    pc = (c + dc) % 2
    way = 1 - 2 * c if sign > 0 else 2 * pc - 1
    px, py, pz = (x + way * dx + 4) % 4, (y + way * dy + 4) % 4, (z + way * dz + 4) % 4
    return {"sp": (pz * 4 + py) * 2 + pc, "tp": px}


def offset_of(e):
    x, y, z, c = place()
    ex, ec, ey, ez = e & 3, (e >> 2) & 1, (e >> 3) & 3, e >> 5
    way = 1 - 2 * c
    dz = (way * (ez - z)) & 3
    return ((ec - c) & 1) * 64 + (dz & 1) * 32 + (dz >> 1) * 16 + ((way * (ey - y)) & 3) * 4 + ((way * (ex - x)) & 3)


def slot_rows(mine, other, earlier, axis):
    return jnp.sum(((mine == other) & earlier).astype(f32), axis=axis, keepdims=True).astype(jnp.int32)


def silu(values):
    return values * (1.0 / (1.0 + jnp.exp(-values)))


def across(row):
    n = row.shape[1]
    same = lax.broadcasted_iota(jnp.int32, (n, n), 0) == lax.broadcasted_iota(jnp.int32, (n, n), 1)
    return jnp.sum(jnp.where(same, row, jnp.zeros_like(row)), axis=1, keepdims=True)


def along(col):
    n = col.shape[0]
    same = lax.broadcasted_iota(jnp.int32, (n, n), 0) == lax.broadcasted_iota(jnp.int32, (n, n), 1)
    return jnp.sum(jnp.where(same, col, jnp.zeros_like(col)), axis=0, keepdims=True)


def layer_kernel(
    value_hbm,
    gate_in_hbm,
    taps_hbm,
    channel_gain_hbm,
    point_hbm,
    residual_hbm,
    first_gain_hbm,
    second_gain_hbm,
    routes_hbm,
    score_hbm,
    gate_hbm,
    up_hbm,
    down_hbm,
    out_ref,
    taps_ref,
    channel_gain_ref,
    first_gain_ref,
    second_gain_ref,
    routes_ref,
    score_ref,
    stat_send,
    stat_recv,
    value,
    gate_in,
    rim,
    glu,
    conv_send,
    conv_own,
    conv_recv,
    gains,
    point,
    residual,
    act,
    h1,
    stacked,
    gate_w,
    up_w,
    down_w,
    send,
    recv,
    flat,
    hidden,
    answer,
    back_send,
    back_recv,
    pick,
    total,
    in_sem,
    small_sem,
    w_sem,
    rim_sem,
    stat_sem,
    gain_sem,
    conv_sem,
    send_sem,
    recv_sem,
    back_send_sem,
    back_recv_sem,
    word,
):
    inputs = [
        pltpu.make_async_copy(value_hbm, value, in_sem.at[0]),
        pltpu.make_async_copy(gate_in_hbm, gate_in, in_sem.at[1]),
        pltpu.make_async_copy(taps_hbm, taps_ref, in_sem.at[2]),
    ]
    small = [
        pltpu.make_async_copy(src, dst, small_sem.at[i])
        for i, (src, dst) in enumerate(
            (
                (channel_gain_hbm, channel_gain_ref),
                (routes_hbm, routes_ref),
                (score_hbm, score_ref),
                (first_gain_hbm, first_gain_ref),
                (second_gain_hbm, second_gain_ref),
            )
        )
    ]
    weights = [
        pltpu.make_async_copy(point_hbm, point, w_sem.at[0]),
        pltpu.make_async_copy(residual_hbm, residual, w_sem.at[1]),
        pltpu.make_async_copy(gate_hbm.at[0], gate_w, w_sem.at[2]),
        pltpu.make_async_copy(up_hbm.at[0], up_w, w_sem.at[3]),
        pltpu.make_async_copy(down_hbm.at[0], down_w, w_sem.at[4]),
    ]
    for copy in inputs + small:
        copy.start()
    barrier = pltpu.get_barrier_semaphore()

    sp, x = lax.axis_index("sp"), lax.axis_index("tp")
    x_line = [partner(d, 1) for d in (1, 2, 3)]
    y_line = [partner(4 * d, 1) for d in (1, 2, 3)]
    z_line = [partner(n, 1) for n in (16, 32, 48)]
    twin = partner(HALF, 1)
    beside = {"sp": (sp + 2 * (sp % 2) - 1 + 32) % 32, "tp": x}
    met = x_line + y_line + z_line + [twin, beside]
    for device in met:
        pl.semaphore_signal(barrier, inc=1, device_id=device, device_id_type=MESH)

    def spread_word(i, line):
        for device in line:
            pl.semaphore_signal(word.at[i], inc=1, device_id=device, device_id_type=MESH)

    rows, quarter = conv_own.shape
    width = quarter * QUARTERS
    taps_n = taps_ref.shape[0]
    lanes = glu.shape[3]
    chunks = quarter // lanes
    lead = glu.shape[2] - rows

    def put_glu(block, values, start):
        for cc in range(chunks):
            glu[block, cc, start : start + values.shape[0], :] = values[:, cc * lanes : (cc + 1) * lanes]

    for copy in inputs:
        copy.wait()
    for copy in weights:
        copy.start()
    for p in range(4):
        own = slice(p * rows, (p + 1) * rows)
        gated = value[own, :].astype(f32) * (1.0 / (1.0 + jnp.exp(-gate_in[own, :].astype(f32))))
        put_glu(p, gated, lead)
        if p < 3:
            put_glu(p + 1, gated[rows - lead :], 0)

    def convolve(p, into, first_row, end):
        one = two = jnp.zeros((end - first_row, 1), f32)
        for cc in range(chunks):
            cols = slice(cc * lanes, (cc + 1) * lanes)
            sum_ = jnp.zeros((end - first_row, lanes), f32)
            for j in range(taps_n):
                start = first_row + lead - taps_n + 1 + j
                sum_ = sum_ + taps_ref[j : j + 1, cols] * glu[p, cc, pl.ds(start, end - first_row), :]
            into[first_row:end, cols] = sum_.astype(bf16)
            one = one + jnp.sum(sum_, axis=1, keepdims=True)
            two = two + jnp.sum(sum_ * sum_, axis=1, keepdims=True)
        return one, two

    ahead = (2, 1, 3)
    order = [(x + d) % 4 for d in ahead] + [x]

    def conv_to(k, first_row, end):
        return pltpu.make_async_remote_copy(
            src_ref=conv_send.at[k, pl.ds(first_row, end - first_row)],
            dst_ref=conv_recv.at[3 - ahead[k], pl.ds(first_row, end - first_row)],
            send_sem=conv_sem.at[3],
            recv_sem=conv_sem.at[3 - ahead[k]],
            device_id={"sp": sp, "tp": order[k]},
            device_id_type=MESH,
        )

    def stat_to(k):
        return pltpu.make_async_remote_copy(
            src_ref=stat_send.at[k],
            dst_ref=stat_recv.at[3 - ahead[k]],
            send_sem=stat_sem.at[0],
            recv_sem=stat_sem.at[1],
            device_id={"sp": sp, "tp": order[k]},
            device_id_type=MESH,
        )

    def gain_to(d):
        return pltpu.make_async_remote_copy(
            src_ref=channel_gain_ref,
            dst_ref=gains.at[3 - d],
            send_sem=gain_sem.at[0],
            recv_sem=gain_sem.at[1],
            device_id={"sp": sp, "tp": (x + d) % 4},
            device_id_type=MESH,
        )

    total_rows = value.shape[0]
    behind = {"sp": (sp + 1) % 32, "tp": x}
    rims = [
        pltpu.make_async_remote_copy(
            src_ref=ref.at[pl.ds(total_rows - lead, lead)],
            dst_ref=rim.at[i],
            send_sem=rim_sem.at[0],
            recv_sem=rim_sem.at[1],
            device_id=behind,
            device_id_type=MESH,
        )
        for i, ref in enumerate((value, gate_in))
    ]
    lower = [convolve(order[0], conv_send.at[0], lead, rows)]
    pl.semaphore_wait(barrier, len(met))
    for copy in rims:
        copy.start()
    conv_to(0, lead, rows).start()
    for k in (1, 2):
        lower.append(convolve(order[k], conv_send.at[k], lead, rows))
        conv_to(k, lead, rows).start()
    small[0].wait()
    for d in range(1, 4):
        gain_to(d).start()
    spread_word(0, y_line)
    lower.append(convolve(x, conv_own, lead, rows))
    pltpu.make_async_copy(rim, rim, rim_sem.at[1]).wait()
    gated = rim[0].astype(f32) * (1.0 / (1.0 + jnp.exp(-rim[1].astype(f32))))
    put_glu(0, jnp.where(sp > 0, gated, jnp.zeros_like(gated)), 0)
    for k in range(3):
        upper = convolve(order[k], conv_send.at[k], 0, lead)
        for i in range(2):
            stat_send[k, i : i + 1, :] = along(jnp.concatenate([upper[i], lower[k][i]], axis=0))
        stat_to(k).start()
        conv_to(k, 0, lead).start()
    upper = convolve(x, conv_own, 0, lead)
    sums = [along(jnp.concatenate([upper[i], lower[3][i]], axis=0)) for i in range(2)]
    pl.semaphore_wait(word.at[0], 3)
    spread_word(1, z_line)
    for copy in small[1:]:
        copy.wait()

    row = [routes_ref[k : k + 1, :] for k in range(2)]
    col = [across(r) for r in row]
    r_id = lax.broadcasted_iota(jnp.int32, (rows, rows), 0)
    c_id = lax.broadcasted_iota(jnp.int32, (rows, rows), 1)
    every = r_id >= 0
    before_l = [
        slot_rows(row[0], col[0], r_id < c_id, 0),
        slot_rows(row[1], col[0], every, 0) + slot_rows(row[1], col[1], r_id < c_id, 0),
    ]
    before_s = [
        slot_rows(col[0], row[0], c_id < r_id, 1),
        slot_rows(col[1], row[0], every, 1) + slot_rows(col[1], row[1], c_id < r_id, 1),
    ]
    where_l = [offset_of(row[k]) * BLOCK + before_l[k] for k in range(2)]
    where_s = [offset_of(col[k]) * BLOCK + before_s[k] for k in range(2)]
    key_l = [jnp.concatenate([where_l[k] + q * SLOTS for q in range(QUARTERS)], axis=1) for k in range(2)]

    def choose(b, carry):
        ids = lax.broadcasted_iota(jnp.int32, (rows, PEERS * BLOCK), 1)
        k, q = b // QUARTERS, b % QUARTERS
        key = jnp.where(k == 0, where_s[0], where_s[1]) + q * SLOTS
        pick[pl.ds(pl.multiple_of(b * rows, rows), rows)] = (ids == key).astype(f32).astype(bf16)
        return carry

    lax.fori_loop(0, QUARTERS, choose, 0)
    pl.semaphore_wait(word.at[1], 3)
    spread_word(2, [twin])
    lax.fori_loop(QUARTERS, 2 * QUARTERS, choose, 0)

    pltpu.make_async_copy(gains, gains, gain_sem.at[1]).wait()
    pltpu.make_async_copy(stat_recv, stat_recv, stat_sem.at[1]).wait()
    for k in range(3):
        sums = [sums[i] + stat_recv[k, i : i + 1, :] for i in range(2)]
    middle = sums[0] / width
    spread = sums[1] / width - middle * middle
    scale = across(lax.rsqrt(spread + 1e-05))
    middle = across(middle)
    for copy in weights[:2]:
        copy.wait()
    for i in (0, 2, 3, 1):
        if i > 0:
            pltpu.make_async_copy(conv_recv.at[i - 1], conv_recv.at[i - 1], conv_sem.at[i - 1]).wait()
        values = conv_own[...] if i == 0 else conv_recv[i - 1]
        gain = channel_gain_ref[...] if i == 0 else gains[i - 1]
        act[...] = silu((values.astype(f32) - middle) * scale * gain).astype(bf16)
        block = (x + i) % 4

        def mix(b, carry):
            cols = pl.ds(pl.multiple_of(b * quarter, quarter), quarter)
            part = jnp.dot(
                act[...],
                point[pl.ds(pl.multiple_of(block * quarter, quarter), quarter), cols],
                preferred_element_type=f32,
            )
            h1[b] = (residual_scale * residual[:, cols].astype(f32) if i == 0 else h1[b]) + part
            return carry

        lax.fori_loop(0, QUARTERS, mix, 0)
    middle = sum(jnp.sum(h1[q], axis=1, keepdims=True) for q in range(QUARTERS)) / width
    centred = [h1[q] - middle for q in range(QUARTERS)]
    spread = sum(jnp.sum(v * v, axis=1, keepdims=True) for v in centred) / width
    scale = lax.rsqrt(spread + 1e-05)
    for q in range(QUARTERS):
        cols = slice(q * quarter, (q + 1) * quarter)
        stacked[pl.ds(q * rows, rows), :] = (centred[q] * scale * first_gain_ref[:, cols]).astype(bf16)

    def fill(b, carry):
        ids = lax.broadcasted_iota(jnp.int32, (512, QUARTERS * rows), 0) + b * 512
        chosen = ((ids == key_l[0]) | (ids == key_l[1])).astype(f32).astype(bf16)
        picked = jnp.dot(chosen, stacked[...], preferred_element_type=f32).astype(bf16)
        send[pl.ds(pl.multiple_of(b * 32, 32), 32)] = picked.reshape(32, BLOCK, quarter)
        return carry

    pl.semaphore_wait(word.at[2], 1)
    def dispatch_to(n, h):
        return pltpu.make_async_remote_copy(
            src_ref=send.at[n],
            dst_ref=recv.at[n],
            send_sem=send_sem,
            recv_sem=recv_sem.at[h],
            device_id=partner(n, 1),
            device_id_type=MESH,
        )

    def answer_to(n, h):
        return pltpu.make_async_remote_copy(
            src_ref=back_send.at[n],
            dst_ref=back_recv.at[n],
            send_sem=back_send_sem,
            recv_sem=back_recv_sem.at[h],
            device_id=partner(n, -1),
            device_id_type=MESH,
        )

    recv_group = 512 // BLOCK
    for h, part in enumerate(PARTS):
        lax.fori_loop(part[0] // recv_group, sum(part) // recv_group, fill, 0)
        for n in far_to_near(part):
            dispatch_to(n, h).start()
    recv[0] = send[0]

    i = lax.broadcasted_iota(jnp.int32, (256, 256), 0)
    j = lax.broadcasted_iota(jnp.int32, (256, 256), 1)
    to_flat = (((i // 4) % 16) * 16 + (i // 64) * 4 + i % 4 == j).astype(f32).astype(bf16)
    to_block = (((j // 4) % 16) * 16 + (j // 64) * 4 + j % 4 == i).astype(f32).astype(bf16)

    for h, (start, count) in enumerate(PARTS):
        own = 1 if h == 0 else 0
        m = count * SLOTS
        landed = recv.at[pl.ds(start + own, count - own)]
        pltpu.make_async_copy(landed, landed, recv_sem.at[h]).wait()
        for g in range(count // 16):
            block = recv[pl.ds(start + g * 16, 16)].reshape(256, quarter)
            moved = jnp.dot(to_flat, block, preferred_element_type=f32).astype(bf16)
            for q in range(QUARTERS):
                flat[pl.ds(g * 64, 64), pl.ds(q * quarter, quarter)] = moved[q * 64 : (q + 1) * 64]
        if h == 0:
            for copy in weights[2:]:
                copy.wait()

        def hide(b, carry):
            cols = pl.ds(pl.multiple_of(b * 256, 256), 256)
            gate = jnp.dot(flat[:m], gate_w[:, cols], preferred_element_type=f32)
            upper = jnp.dot(flat[:m], up_w[:, cols], preferred_element_type=f32)
            hidden[:m, cols] = (silu(gate) * upper).astype(bf16)
            return carry

        lax.fori_loop(0, hidden.shape[1] // 256, hide, 0)
        for q in range(QUARTERS):
            cols = pl.ds(q * quarter, quarter)
            result = jnp.dot(hidden[:m], down_w[:, cols], preferred_element_type=f32).astype(bf16)
            for g in range(count // 16):
                answer[g, pl.ds(q * 64, 64), :] = result[g * 64 : (g + 1) * 64]
        for g in range(count // 16):
            moved = jnp.dot(to_block, answer[g], preferred_element_type=f32).astype(bf16)
            back_send[pl.ds(start + g * 16, 16)] = moved.reshape(16, BLOCK, quarter)
        if h == 0:
            back_recv[0] = back_send[0]
        for n in far_to_near((start, count)):
            answer_to(n, h).start()

    for h, (start, count) in enumerate(PARTS):
        own = 1 if h == 0 else 0
        landed = back_recv.at[pl.ds(start + own, count - own)]
        pltpu.make_async_copy(landed, landed, back_recv_sem.at[h]).wait()
        block = back_recv[pl.ds(start, count)].reshape(count * BLOCK, quarter)
        part = jnp.dot(pick[:, pl.ds(start * BLOCK, count * BLOCK)], block, preferred_element_type=f32)
        total[...] = part if h == 0 else total[...] + part

    share = [across(score_ref[k : k + 1, :] / (score_ref[0:1, :] + score_ref[1:2, :])) for k in range(2)]
    mixed = []
    for q in range(QUARTERS):
        base = residual_scale * stacked[pl.ds(q * rows, rows), :].astype(f32)
        one = total[pl.ds(q * rows, rows), :] * share[0]
        two = total[pl.ds((QUARTERS + q) * rows, rows), :] * share[1]
        mixed.append(base + (one + two))
    middle = sum(jnp.sum(m, axis=1, keepdims=True) for m in mixed) / width
    mixed = [m - middle for m in mixed]
    spread = sum(jnp.sum(m * m, axis=1, keepdims=True) for m in mixed) / width
    scale = lax.rsqrt(spread + 1e-05)
    for q in range(QUARTERS):
        cols = slice(q * quarter, (q + 1) * quarter)
        out_ref[:, cols] = (mixed[q] * scale * second_gain_ref[:, cols]).astype(bf16)

    for copy in rims:
        copy.wait_send()
    for k in range(3):
        conv_to(k, 0, rows).wait_send()
        stat_to(k).wait_send()
    for d in range(1, 4):
        gain_to(d).wait_send()
    sent = send.at[pl.ds(1, PEERS - 1)]
    pltpu.make_async_copy(sent, sent, send_sem).wait()
    sent = back_send.at[pl.ds(1, PEERS - 1)]
    pltpu.make_async_copy(sent, sent, back_send_sem).wait()


def per_device(
    conv_value,
    conv_gate,
    conv_taps,
    channel_gain,
    point_weight,
    residual_in,
    first_gain,
    second_gain,
    routes,
    route_score,
    expert_gate,
    expert_up,
    expert_down,
):
    rows, width = residual_in.shape
    inner = expert_gate.shape[2]
    tokens, quarter = conv_value.shape
    lanes = 128
    lead = -(-(conv_taps.shape[0] - 1) // 16) * 16
    vmem = pl.BlockSpec(memory_space=pltpu.VMEM)
    hbm = pl.BlockSpec(memory_space=pl.ANY)
    blocks = pltpu.VMEM((PEERS, BLOCK, quarter), bf16)
    dma = pltpu.SemaphoreType.DMA
    return pl.pallas_call(
        layer_kernel,
        out_shape=pltpu.VMEM((rows, width), bf16),
        in_specs=[hbm] * 13,
        out_specs=vmem,
        scratch_shapes=[
            pltpu.VMEM(conv_taps.shape, f32),
            pltpu.VMEM((1, quarter), f32),
            pltpu.VMEM((1, width), f32),
            pltpu.VMEM((1, width), f32),
            pltpu.VMEM((2, rows), jnp.int32),
            pltpu.VMEM((2, rows), f32),
            pltpu.VMEM((3, 2, rows), f32),
            pltpu.VMEM((3, 2, rows), f32),
            pltpu.VMEM((tokens, quarter), bf16),
            pltpu.VMEM((tokens, quarter), bf16),
            pltpu.VMEM((2, lead, quarter), bf16),
            pltpu.VMEM((4, quarter // lanes, lead + rows, lanes), f32),
            pltpu.VMEM((3, rows, quarter), bf16),
            pltpu.VMEM((rows, quarter), bf16),
            pltpu.VMEM((3, rows, quarter), bf16),
            pltpu.VMEM((3, 1, quarter), f32),
            pltpu.VMEM((width, width), bf16),
            pltpu.VMEM((rows, width), bf16),
            pltpu.VMEM((rows, quarter), bf16),
            pltpu.VMEM((QUARTERS, rows, quarter), f32),
            pltpu.VMEM((QUARTERS * rows, quarter), bf16),
            pltpu.VMEM((width, inner), bf16),
            pltpu.VMEM((width, inner), bf16),
            pltpu.VMEM((inner, width), bf16),
            blocks,
            blocks,
            pltpu.VMEM((HALF * SLOTS, width), bf16),
            pltpu.VMEM((HALF * SLOTS, inner), bf16),
            pltpu.VMEM((4, 256, quarter), bf16),
            blocks,
            blocks,
            pltpu.VMEM((2 * QUARTERS * rows, PEERS * BLOCK), bf16),
            pltpu.VMEM((2 * QUARTERS * rows, quarter), f32),
            dma((3,)),
            dma((5,)),
            dma((5,)),
            dma((2,)),
            dma((2,)),
            dma((2,)),
            dma((4,)),
            dma,
            dma((4,)),
            dma,
            dma((4,)),
            pltpu.SemaphoreType.REGULAR((3,)),
        ],
        compiler_params=pltpu.CompilerParams(
            collective_id=1, has_side_effects=True, vmem_limit_bytes=60 * 1024 * 1024
        ),
        name="layer",
    )(
        conv_value,
        conv_gate,
        conv_taps,
        channel_gain.reshape(1, -1),
        point_weight,
        residual_in,
        first_gain.reshape(1, -1),
        second_gain.reshape(1, -1),
        routes.T,
        route_score.T,
        expert_gate,
        expert_up,
        expert_down,
    )


def solution(mesh):
    in_specs = (
        P("sp", "tp"),
        P("sp", "tp"),
        P(None, "tp"),
        P("tp"),
        P(),
        P(("sp", "tp"), None),
        P(),
        P(),
        P(("sp", "tp"), None),
        P(("sp", "tp"), None),
        P(("sp", "tp"), None, None),
        P(("sp", "tp"), None, None),
        P(("sp", "tp"), None, None),
    )
    out_specs = P(("sp", "tp"), None)
    return jax.shard_map(
        per_device, mesh=mesh, in_specs=in_specs, out_specs=out_specs, check_vma=False
    )
```

```python
import functools

import jax
import jax.numpy as jnp
from jax import lax
from jax.experimental import pallas as pl
from jax.experimental.pallas import tpu as pltpu
from jax.sharding import PartitionSpec as P

residual_scale = 8.0**0.25
MESH = pl.DeviceIdType.MESH
f32, bf16 = jnp.float32, jnp.bfloat16

PEERS, SLOTS, QUARTERS = 128, 4, 4
BLOCK = SLOTS * QUARTERS
HALF = PEERS // 2
PARTS = ((0, 32), (32, 32), (64, 32), (96, 32))


def far_to_near(part):
    first, count = part
    hops = (0, 1, 2, 1)
    return [n for n in (first + (k * 37) % count for k in range(count)) if n > 0]


def place():
    sp, x = lax.axis_index("sp"), lax.axis_index("tp")
    return x, (sp // 2) % 4, sp // 8, sp % 2


def partner(n, sign):
    x, y, z, c = place()
    dx, dy, dz, dc = n % 4, (n // 4) % 4, (n // 16) % 2 * 2 + (n // 32) % 2, n // 64
    pc = (c + dc) % 2
    way = 1 - 2 * c if sign > 0 else 2 * pc - 1
    px, py, pz = (x + way * dx + 4) % 4, (y + way * dy + 4) % 4, (z + way * dz + 4) % 4
    return {"sp": (pz * 4 + py) * 2 + pc, "tp": px}


def offset_of(e):
    x, y, z, c = place()
    ex, ec, ey, ez = e & 3, (e >> 2) & 1, (e >> 3) & 3, e >> 5
    way = 1 - 2 * c
    dz = (way * (ez - z)) & 3
    return ((ec - c) & 1) * 64 + (dz & 1) * 32 + (dz >> 1) * 16 + ((way * (ey - y)) & 3) * 4 + ((way * (ex - x)) & 3)


def slot_rows(mine, other, earlier, axis):
    return jnp.sum(((mine == other) & earlier).astype(f32), axis=axis, keepdims=True).astype(jnp.int32)


def silu(values):
    return values * (1.0 / (1.0 + jnp.exp(-values)))


def across(row):
    n = row.shape[1]
    same = lax.broadcasted_iota(jnp.int32, (n, n), 0) == lax.broadcasted_iota(jnp.int32, (n, n), 1)
    return jnp.sum(jnp.where(same, row, jnp.zeros_like(row)), axis=1, keepdims=True)


def along(col):
    n = col.shape[0]
    same = lax.broadcasted_iota(jnp.int32, (n, n), 0) == lax.broadcasted_iota(jnp.int32, (n, n), 1)
    return jnp.sum(jnp.where(same, col, jnp.zeros_like(col)), axis=0, keepdims=True)


def layer_kernel(
    value_hbm,
    gate_in_hbm,
    taps_hbm,
    channel_gain_hbm,
    point_hbm,
    residual_hbm,
    first_gain_hbm,
    second_gain_hbm,
    routes_hbm,
    score_hbm,
    gate_hbm,
    up_hbm,
    down_hbm,
    out_ref,
    taps_ref,
    channel_gain_ref,
    first_gain_ref,
    second_gain_ref,
    routes_ref,
    score_ref,
    stat_send,
    stat_recv,
    value,
    gate_in,
    rim,
    glu,
    conv_send,
    conv_own,
    conv_recv,
    gains,
    point,
    residual,
    act,
    h1,
    stacked,
    gate_w,
    up_w,
    down_w,
    send,
    recv,
    flat,
    hidden,
    answer,
    back_send,
    back_recv,
    pick,
    total,
    in_sem,
    small_sem,
    w_sem,
    rim_sem,
    stat_sem,
    gain_sem,
    conv_sem,
    send_sem,
    recv_sem,
    back_send_sem,
    back_recv_sem,
    word,
):
    inputs = [
        pltpu.make_async_copy(value_hbm, value, in_sem.at[0]),
        pltpu.make_async_copy(gate_in_hbm, gate_in, in_sem.at[1]),
        pltpu.make_async_copy(taps_hbm, taps_ref, in_sem.at[2]),
    ]
    small = [
        pltpu.make_async_copy(src, dst, small_sem.at[i])
        for i, (src, dst) in enumerate(
            (
                (channel_gain_hbm, channel_gain_ref),
                (routes_hbm, routes_ref),
                (score_hbm, score_ref),
                (first_gain_hbm, first_gain_ref),
                (second_gain_hbm, second_gain_ref),
            )
        )
    ]
    weights = [
        pltpu.make_async_copy(point_hbm, point, w_sem.at[0]),
        pltpu.make_async_copy(residual_hbm, residual, w_sem.at[1]),
        pltpu.make_async_copy(gate_hbm.at[0], gate_w, w_sem.at[2]),
        pltpu.make_async_copy(up_hbm.at[0], up_w, w_sem.at[3]),
        pltpu.make_async_copy(down_hbm.at[0], down_w, w_sem.at[4]),
    ]
    for copy in inputs + small:
        copy.start()
    barrier = pltpu.get_barrier_semaphore()

    sp, x = lax.axis_index("sp"), lax.axis_index("tp")
    x_line = [partner(d, 1) for d in (1, 2, 3)]
    y_line = [partner(4 * d, 1) for d in (1, 2, 3)]
    z_line = [partner(n, 1) for n in (16, 32, 48)]
    twin = partner(HALF, 1)
    beside = {"sp": (sp + 2 * (sp % 2) - 1 + 32) % 32, "tp": x}
    met = x_line + y_line + z_line + [twin, beside]
    for device in met:
        pl.semaphore_signal(barrier, inc=1, device_id=device, device_id_type=MESH)

    def spread_word(i, line):
        for device in line:
            pl.semaphore_signal(word.at[i], inc=1, device_id=device, device_id_type=MESH)

    rows, quarter = conv_own.shape
    width = quarter * QUARTERS
    taps_n = taps_ref.shape[0]
    lanes = glu.shape[3]
    chunks = quarter // lanes
    lead = glu.shape[2] - rows

    def put_glu(block, values, start):
        for cc in range(chunks):
            glu[block, cc, start : start + values.shape[0], :] = values[:, cc * lanes : (cc + 1) * lanes]

    for copy in inputs:
        copy.wait()
    for copy in weights:
        copy.start()
    for p in range(4):
        own = slice(p * rows, (p + 1) * rows)
        gated = value[own, :].astype(f32) * (1.0 / (1.0 + jnp.exp(-gate_in[own, :].astype(f32))))
        put_glu(p, gated, lead)
        if p < 3:
            put_glu(p + 1, gated[rows - lead :], 0)

    def convolve(p, into, first_row, end):
        one = two = jnp.zeros((end - first_row, 1), f32)
        for cc in range(chunks):
            cols = slice(cc * lanes, (cc + 1) * lanes)
            sum_ = jnp.zeros((end - first_row, lanes), f32)
            for j in range(taps_n):
                start = first_row + lead - taps_n + 1 + j
                sum_ = sum_ + taps_ref[j : j + 1, cols] * glu[p, cc, pl.ds(start, end - first_row), :]
            into[first_row:end, cols] = sum_.astype(bf16)
            one = one + jnp.sum(sum_, axis=1, keepdims=True)
            two = two + jnp.sum(sum_ * sum_, axis=1, keepdims=True)
        return one, two

    ahead = (2, 1, 3)
    order = [(x + d) % 4 for d in ahead] + [x]

    def conv_to(k, first_row, end):
        return pltpu.make_async_remote_copy(
            src_ref=conv_send.at[k, pl.ds(first_row, end - first_row)],
            dst_ref=conv_recv.at[3 - ahead[k], pl.ds(first_row, end - first_row)],
            send_sem=conv_sem.at[3],
            recv_sem=conv_sem.at[3 - ahead[k]],
            device_id={"sp": sp, "tp": order[k]},
            device_id_type=MESH,
        )

    def stat_to(k):
        return pltpu.make_async_remote_copy(
            src_ref=stat_send.at[k],
            dst_ref=stat_recv.at[3 - ahead[k]],
            send_sem=stat_sem.at[0],
            recv_sem=stat_sem.at[1],
            device_id={"sp": sp, "tp": order[k]},
            device_id_type=MESH,
        )

    def gain_to(d):
        return pltpu.make_async_remote_copy(
            src_ref=channel_gain_ref,
            dst_ref=gains.at[3 - d],
            send_sem=gain_sem.at[0],
            recv_sem=gain_sem.at[1],
            device_id={"sp": sp, "tp": (x + d) % 4},
            device_id_type=MESH,
        )

    total_rows = value.shape[0]
    behind = {"sp": (sp + 1) % 32, "tp": x}
    rims = [
        pltpu.make_async_remote_copy(
            src_ref=ref.at[pl.ds(total_rows - lead, lead)],
            dst_ref=rim.at[i],
            send_sem=rim_sem.at[0],
            recv_sem=rim_sem.at[1],
            device_id=behind,
            device_id_type=MESH,
        )
        for i, ref in enumerate((value, gate_in))
    ]
    lower = [convolve(order[0], conv_send.at[0], lead, rows)]
    pl.semaphore_wait(barrier, len(met))
    for copy in rims:
        copy.start()
    conv_to(0, lead, rows).start()
    for k in (1, 2):
        lower.append(convolve(order[k], conv_send.at[k], lead, rows))
        conv_to(k, lead, rows).start()
    small[0].wait()
    for d in range(1, 4):
        gain_to(d).start()
    spread_word(0, y_line)
    lower.append(convolve(x, conv_own, lead, rows))
    pltpu.make_async_copy(rim, rim, rim_sem.at[1]).wait()
    gated = rim[0].astype(f32) * (1.0 / (1.0 + jnp.exp(-rim[1].astype(f32))))
    put_glu(0, jnp.where(sp > 0, gated, jnp.zeros_like(gated)), 0)
    for k in range(3):
        upper = convolve(order[k], conv_send.at[k], 0, lead)
        for i in range(2):
            stat_send[k, i : i + 1, :] = along(jnp.concatenate([upper[i], lower[k][i]], axis=0))
        stat_to(k).start()
        conv_to(k, 0, lead).start()
    upper = convolve(x, conv_own, 0, lead)
    sums = [along(jnp.concatenate([upper[i], lower[3][i]], axis=0)) for i in range(2)]
    pl.semaphore_wait(word.at[0], 3)
    spread_word(1, z_line)
    for copy in small[1:]:
        copy.wait()

    row = [routes_ref[k : k + 1, :] for k in range(2)]
    col = [across(r) for r in row]
    r_id = lax.broadcasted_iota(jnp.int32, (rows, rows), 0)
    c_id = lax.broadcasted_iota(jnp.int32, (rows, rows), 1)
    every = r_id >= 0
    before_l = [
        slot_rows(row[0], col[0], r_id < c_id, 0),
        slot_rows(row[1], col[0], every, 0) + slot_rows(row[1], col[1], r_id < c_id, 0),
    ]
    before_s = [
        slot_rows(col[0], row[0], c_id < r_id, 1),
        slot_rows(col[1], row[0], every, 1) + slot_rows(col[1], row[1], c_id < r_id, 1),
    ]
    where_l = [offset_of(row[k]) * BLOCK + before_l[k] for k in range(2)]
    where_s = [offset_of(col[k]) * BLOCK + before_s[k] for k in range(2)]
    key_l = [jnp.concatenate([where_l[k] + q * SLOTS for q in range(QUARTERS)], axis=1) for k in range(2)]

    def choose(b, carry):
        ids = lax.broadcasted_iota(jnp.int32, (rows, PEERS * BLOCK), 1)
        k, q = b // QUARTERS, b % QUARTERS
        key = jnp.where(k == 0, where_s[0], where_s[1]) + q * SLOTS
        pick[pl.ds(pl.multiple_of(b * rows, rows), rows)] = (ids == key).astype(f32).astype(bf16)
        return carry

    lax.fori_loop(0, QUARTERS, choose, 0)
    pl.semaphore_wait(word.at[1], 3)
    spread_word(2, [twin])
    lax.fori_loop(QUARTERS, 2 * QUARTERS, choose, 0)

    pltpu.make_async_copy(gains, gains, gain_sem.at[1]).wait()
    pltpu.make_async_copy(stat_recv, stat_recv, stat_sem.at[1]).wait()
    for k in range(3):
        sums = [sums[i] + stat_recv[k, i : i + 1, :] for i in range(2)]
    middle = sums[0] / width
    spread = sums[1] / width - middle * middle
    scale = across(lax.rsqrt(spread + 1e-05))
    middle = across(middle)
    for copy in weights[:2]:
        copy.wait()
    for i in (0, 2, 3, 1):
        if i > 0:
            pltpu.make_async_copy(conv_recv.at[i - 1], conv_recv.at[i - 1], conv_sem.at[i - 1]).wait()
        values = conv_own[...] if i == 0 else conv_recv[i - 1]
        gain = channel_gain_ref[...] if i == 0 else gains[i - 1]
        act[...] = silu((values.astype(f32) - middle) * scale * gain).astype(bf16)
        block = (x + i) % 4

        for b in range(QUARTERS):
            cols = slice(b * quarter, (b + 1) * quarter)
            part = jnp.dot(
                act[...],
                point[pl.ds(pl.multiple_of(block * quarter, quarter), quarter), cols],
                preferred_element_type=f32,
            )
            h1[b] = (residual_scale * residual[:, cols].astype(f32) if i == 0 else h1[b]) + part
    middle = sum(jnp.sum(h1[q], axis=1, keepdims=True) for q in range(QUARTERS)) / width
    centred = [h1[q] - middle for q in range(QUARTERS)]
    spread = sum(jnp.sum(v * v, axis=1, keepdims=True) for v in centred) / width
    scale = lax.rsqrt(spread + 1e-05)
    for q in range(QUARTERS):
        cols = slice(q * quarter, (q + 1) * quarter)
        stacked[pl.ds(q * rows, rows), :] = (centred[q] * scale * first_gain_ref[:, cols]).astype(bf16)

    def fill(b, carry):
        ids = lax.broadcasted_iota(jnp.int32, (512, QUARTERS * rows), 0) + b * 512
        chosen = ((ids == key_l[0]) | (ids == key_l[1])).astype(f32).astype(bf16)
        picked = jnp.dot(chosen, stacked[...], preferred_element_type=f32).astype(bf16)
        send[pl.ds(pl.multiple_of(b * 32, 32), 32)] = picked.reshape(32, BLOCK, quarter)
        return carry

    pl.semaphore_wait(word.at[2], 1)
    def dispatch_to(n, h):
        return pltpu.make_async_remote_copy(
            src_ref=send.at[n],
            dst_ref=recv.at[n],
            send_sem=send_sem,
            recv_sem=recv_sem.at[h],
            device_id=partner(n, 1),
            device_id_type=MESH,
        )

    def answer_to(n, h):
        return pltpu.make_async_remote_copy(
            src_ref=back_send.at[n],
            dst_ref=back_recv.at[n],
            send_sem=back_send_sem,
            recv_sem=back_recv_sem.at[h],
            device_id=partner(n, -1),
            device_id_type=MESH,
        )

    recv_group = 512 // BLOCK
    for h, part in enumerate(PARTS):
        lax.fori_loop(part[0] // recv_group, sum(part) // recv_group, fill, 0)
        for n in far_to_near(part):
            dispatch_to(n, h).start()
    recv[0] = send[0]

    i = lax.broadcasted_iota(jnp.int32, (256, 256), 0)
    j = lax.broadcasted_iota(jnp.int32, (256, 256), 1)
    to_flat = (((i // 4) % 16) * 16 + (i // 64) * 4 + i % 4 == j).astype(f32).astype(bf16)
    to_block = (((j // 4) % 16) * 16 + (j // 64) * 4 + j % 4 == i).astype(f32).astype(bf16)

    for h, (start, count) in enumerate(PARTS):
        own = 1 if h == 0 else 0
        m = count * SLOTS
        landed = recv.at[pl.ds(start + own, count - own)]
        pltpu.make_async_copy(landed, landed, recv_sem.at[h]).wait()
        for g in range(count // 16):
            block = recv[pl.ds(start + g * 16, 16)].reshape(256, quarter)
            moved = jnp.dot(to_flat, block, preferred_element_type=f32).astype(bf16)
            for q in range(QUARTERS):
                flat[pl.ds(g * 64, 64), pl.ds(q * quarter, quarter)] = moved[q * 64 : (q + 1) * 64]
        if h == 0:
            for copy in weights[2:]:
                copy.wait()

        def hide(b, carry):
            cols = pl.ds(pl.multiple_of(b * 256, 256), 256)
            gate = jnp.dot(flat[:m], gate_w[:, cols], preferred_element_type=f32)
            upper = jnp.dot(flat[:m], up_w[:, cols], preferred_element_type=f32)
            hidden[:m, cols] = (silu(gate) * upper).astype(bf16)
            return carry

        lax.fori_loop(0, hidden.shape[1] // 256, hide, 0)
        for q in range(QUARTERS):
            cols = pl.ds(q * quarter, quarter)
            result = jnp.dot(hidden[:m], down_w[:, cols], preferred_element_type=f32).astype(bf16)
            for g in range(count // 16):
                answer[g, pl.ds(q * 64, 64), :] = result[g * 64 : (g + 1) * 64]
        for g in range(count // 16):
            moved = jnp.dot(to_block, answer[g], preferred_element_type=f32).astype(bf16)
            back_send[pl.ds(start + g * 16, 16)] = moved.reshape(16, BLOCK, quarter)
        if h == 0:
            back_recv[0] = back_send[0]
        for n in far_to_near((start, count)):
            answer_to(n, h).start()

    for h, (start, count) in enumerate(PARTS):
        own = 1 if h == 0 else 0
        landed = back_recv.at[pl.ds(start + own, count - own)]
        pltpu.make_async_copy(landed, landed, back_recv_sem.at[h]).wait()
        block = back_recv[pl.ds(start, count)].reshape(count * BLOCK, quarter)
        part = jnp.dot(pick[:, pl.ds(start * BLOCK, count * BLOCK)], block, preferred_element_type=f32)
        total[...] = part if h == 0 else total[...] + part

    share = [across(score_ref[k : k + 1, :] / (score_ref[0:1, :] + score_ref[1:2, :])) for k in range(2)]
    mixed = []
    for q in range(QUARTERS):
        base = residual_scale * stacked[pl.ds(q * rows, rows), :].astype(f32)
        one = total[pl.ds(q * rows, rows), :] * share[0]
        two = total[pl.ds((QUARTERS + q) * rows, rows), :] * share[1]
        mixed.append(base + (one + two))
    middle = sum(jnp.sum(m, axis=1, keepdims=True) for m in mixed) / width
    mixed = [m - middle for m in mixed]
    spread = sum(jnp.sum(m * m, axis=1, keepdims=True) for m in mixed) / width
    scale = lax.rsqrt(spread + 1e-05)
    for q in range(QUARTERS):
        cols = slice(q * quarter, (q + 1) * quarter)
        out_ref[:, cols] = (mixed[q] * scale * second_gain_ref[:, cols]).astype(bf16)

    for copy in rims:
        copy.wait_send()
    for k in range(3):
        conv_to(k, 0, rows).wait_send()
        stat_to(k).wait_send()
    for d in range(1, 4):
        gain_to(d).wait_send()
    sent = send.at[pl.ds(1, PEERS - 1)]
    pltpu.make_async_copy(sent, sent, send_sem).wait()
    sent = back_send.at[pl.ds(1, PEERS - 1)]
    pltpu.make_async_copy(sent, sent, back_send_sem).wait()


def per_device(
    conv_value,
    conv_gate,
    conv_taps,
    channel_gain,
    point_weight,
    residual_in,
    first_gain,
    second_gain,
    routes,
    route_score,
    expert_gate,
    expert_up,
    expert_down,
):
    rows, width = residual_in.shape
    inner = expert_gate.shape[2]
    tokens, quarter = conv_value.shape
    lanes = 128
    lead = -(-(conv_taps.shape[0] - 1) // 16) * 16
    vmem = pl.BlockSpec(memory_space=pltpu.VMEM)
    hbm = pl.BlockSpec(memory_space=pl.ANY)
    blocks = pltpu.VMEM((PEERS, BLOCK, quarter), bf16)
    dma = pltpu.SemaphoreType.DMA
    return pl.pallas_call(
        layer_kernel,
        out_shape=pltpu.VMEM((rows, width), bf16),
        in_specs=[hbm] * 13,
        out_specs=vmem,
        scratch_shapes=[
            pltpu.VMEM(conv_taps.shape, f32),
            pltpu.VMEM((1, quarter), f32),
            pltpu.VMEM((1, width), f32),
            pltpu.VMEM((1, width), f32),
            pltpu.VMEM((2, rows), jnp.int32),
            pltpu.VMEM((2, rows), f32),
            pltpu.VMEM((3, 2, rows), f32),
            pltpu.VMEM((3, 2, rows), f32),
            pltpu.VMEM((tokens, quarter), bf16),
            pltpu.VMEM((tokens, quarter), bf16),
            pltpu.VMEM((2, lead, quarter), bf16),
            pltpu.VMEM((4, quarter // lanes, lead + rows, lanes), f32),
            pltpu.VMEM((3, rows, quarter), bf16),
            pltpu.VMEM((rows, quarter), bf16),
            pltpu.VMEM((3, rows, quarter), bf16),
            pltpu.VMEM((3, 1, quarter), f32),
            pltpu.VMEM((width, width), bf16),
            pltpu.VMEM((rows, width), bf16),
            pltpu.VMEM((rows, quarter), bf16),
            pltpu.VMEM((QUARTERS, rows, quarter), f32),
            pltpu.VMEM((QUARTERS * rows, quarter), bf16),
            pltpu.VMEM((width, inner), bf16),
            pltpu.VMEM((width, inner), bf16),
            pltpu.VMEM((inner, width), bf16),
            blocks,
            blocks,
            pltpu.VMEM((HALF * SLOTS, width), bf16),
            pltpu.VMEM((HALF * SLOTS, inner), bf16),
            pltpu.VMEM((4, 256, quarter), bf16),
            blocks,
            blocks,
            pltpu.VMEM((2 * QUARTERS * rows, PEERS * BLOCK), bf16),
            pltpu.VMEM((2 * QUARTERS * rows, quarter), f32),
            dma((3,)),
            dma((5,)),
            dma((5,)),
            dma((2,)),
            dma((2,)),
            dma((2,)),
            dma((4,)),
            dma,
            dma((4,)),
            dma,
            dma((4,)),
            pltpu.SemaphoreType.REGULAR((3,)),
        ],
        compiler_params=pltpu.CompilerParams(
            collective_id=1, has_side_effects=True, vmem_limit_bytes=60 * 1024 * 1024
        ),
        name="layer",
    )(
        conv_value,
        conv_gate,
        conv_taps,
        channel_gain.reshape(1, -1),
        point_weight,
        residual_in,
        first_gain.reshape(1, -1),
        second_gain.reshape(1, -1),
        routes.T,
        route_score.T,
        expert_gate,
        expert_up,
        expert_down,
    )


def solution(mesh):
    in_specs = (
        P("sp", "tp"),
        P("sp", "tp"),
        P(None, "tp"),
        P("tp"),
        P(),
        P(("sp", "tp"), None),
        P(),
        P(),
        P(("sp", "tp"), None),
        P(("sp", "tp"), None),
        P(("sp", "tp"), None, None),
        P(("sp", "tp"), None, None),
        P(("sp", "tp"), None, None),
    )
    out_specs = P(("sp", "tp"), None)
    return jax.shard_map(
        per_device, mesh=mesh, in_specs=in_specs, out_specs=out_specs, check_vma=False
    )
```

```python
import functools

import jax
import jax.numpy as jnp
from jax import lax
from jax.experimental import pallas as pl
from jax.experimental.pallas import tpu as pltpu
from jax.sharding import PartitionSpec as P

residual_scale = 8.0**0.25
MESH = pl.DeviceIdType.MESH
f32, bf16 = jnp.float32, jnp.bfloat16

PEERS, SLOTS, QUARTERS = 128, 4, 4
BLOCK = SLOTS * QUARTERS
HALF = PEERS // 2
PARTS = ((0, 32), (32, 32), (64, 32), (96, 32))


def far_to_near(part):
    first, count = part
    hops = (0, 1, 2, 1)
    return [n for n in (first + (k * 37) % count for k in range(count)) if n > 0]


def place():
    sp, x = lax.axis_index("sp"), lax.axis_index("tp")
    return x, (sp // 2) % 4, sp // 8, sp % 2


def partner(n, sign):
    x, y, z, c = place()
    dx, dy, dz, dc = n % 4, (n // 4) % 4, (n // 16) % 2 * 2 + (n // 32) % 2, n // 64
    pc = (c + dc) % 2
    way = 1 - 2 * c if sign > 0 else 2 * pc - 1
    px, py, pz = (x + way * dx + 4) % 4, (y + way * dy + 4) % 4, (z + way * dz + 4) % 4
    return {"sp": (pz * 4 + py) * 2 + pc, "tp": px}


def offset_of(e):
    x, y, z, c = place()
    ex, ec, ey, ez = e & 3, (e >> 2) & 1, (e >> 3) & 3, e >> 5
    way = 1 - 2 * c
    dz = (way * (ez - z)) & 3
    return ((ec - c) & 1) * 64 + (dz & 1) * 32 + (dz >> 1) * 16 + ((way * (ey - y)) & 3) * 4 + ((way * (ex - x)) & 3)


def slot_rows(mine, other, earlier, axis):
    return jnp.sum(((mine == other) & earlier).astype(f32), axis=axis, keepdims=True).astype(jnp.int32)


def silu(values):
    return values * (1.0 / (1.0 + jnp.exp(-values)))


def across(row):
    n = row.shape[1]
    same = lax.broadcasted_iota(jnp.int32, (n, n), 0) == lax.broadcasted_iota(jnp.int32, (n, n), 1)
    return jnp.sum(jnp.where(same, row, jnp.zeros_like(row)), axis=1, keepdims=True)


def along(col):
    n = col.shape[0]
    same = lax.broadcasted_iota(jnp.int32, (n, n), 0) == lax.broadcasted_iota(jnp.int32, (n, n), 1)
    return jnp.sum(jnp.where(same, col, jnp.zeros_like(col)), axis=0, keepdims=True)


def layer_kernel(
    value_hbm,
    gate_in_hbm,
    taps_hbm,
    channel_gain_hbm,
    point_hbm,
    residual_hbm,
    first_gain_hbm,
    second_gain_hbm,
    routes_hbm,
    score_hbm,
    gate_hbm,
    up_hbm,
    down_hbm,
    out_ref,
    taps_ref,
    channel_gain_ref,
    first_gain_ref,
    second_gain_ref,
    routes_ref,
    score_ref,
    stat_send,
    stat_recv,
    value,
    gate_in,
    rim,
    glu,
    conv_send,
    conv_own,
    conv_recv,
    gains,
    point,
    residual,
    act,
    h1,
    stacked,
    gate_w,
    up_w,
    down_w,
    send,
    recv,
    flat,
    hidden,
    answer,
    back_send,
    back_recv,
    pick,
    total,
    in_sem,
    small_sem,
    w_sem,
    rim_sem,
    stat_sem,
    gain_sem,
    conv_sem,
    send_sem,
    recv_sem,
    back_send_sem,
    back_recv_sem,
    word,
):
    inputs = [
        pltpu.make_async_copy(value_hbm, value, in_sem.at[0]),
        pltpu.make_async_copy(gate_in_hbm, gate_in, in_sem.at[1]),
        pltpu.make_async_copy(taps_hbm, taps_ref, in_sem.at[2]),
    ]
    small = [
        pltpu.make_async_copy(src, dst, small_sem.at[i])
        for i, (src, dst) in enumerate(
            (
                (channel_gain_hbm, channel_gain_ref),
                (routes_hbm, routes_ref),
                (score_hbm, score_ref),
                (first_gain_hbm, first_gain_ref),
                (second_gain_hbm, second_gain_ref),
            )
        )
    ]
    weights = [
        pltpu.make_async_copy(point_hbm, point, w_sem.at[0]),
        pltpu.make_async_copy(residual_hbm, residual, w_sem.at[1]),
        pltpu.make_async_copy(gate_hbm.at[0], gate_w, w_sem.at[2]),
        pltpu.make_async_copy(up_hbm.at[0], up_w, w_sem.at[3]),
        pltpu.make_async_copy(down_hbm.at[0], down_w, w_sem.at[4]),
    ]
    for copy in inputs + small:
        copy.start()
    barrier = pltpu.get_barrier_semaphore()

    sp, x = lax.axis_index("sp"), lax.axis_index("tp")
    x_line = [partner(d, 1) for d in (1, 2, 3)]
    y_line = [partner(4 * d, 1) for d in (1, 2, 3)]
    z_line = [partner(n, 1) for n in (16, 32, 48)]
    twin = partner(HALF, 1)
    beside = {"sp": (sp + 2 * (sp % 2) - 1 + 32) % 32, "tp": x}
    met = x_line + y_line + z_line + [twin, beside]
    for device in met:
        pl.semaphore_signal(barrier, inc=1, device_id=device, device_id_type=MESH)

    def spread_word(i, line):
        for device in line:
            pl.semaphore_signal(word.at[i], inc=1, device_id=device, device_id_type=MESH)

    rows, quarter = conv_own.shape
    width = quarter * QUARTERS
    taps_n = taps_ref.shape[0]
    lanes = glu.shape[3]
    chunks = quarter // lanes
    lead = glu.shape[2] - rows

    def put_glu(block, values, start):
        for cc in range(chunks):
            glu[block, cc, start : start + values.shape[0], :] = values[:, cc * lanes : (cc + 1) * lanes]

    for copy in inputs:
        copy.wait()
    for copy in weights:
        copy.start()
    for p in range(4):
        own = slice(p * rows, (p + 1) * rows)
        gated = value[own, :].astype(f32) * (1.0 / (1.0 + jnp.exp(-gate_in[own, :].astype(f32))))
        put_glu(p, gated, lead)
        if p < 3:
            put_glu(p + 1, gated[rows - lead :], 0)

    def convolve(p, into, first_row, end):
        one = two = jnp.zeros((end - first_row, 1), f32)
        for cc in range(chunks):
            cols = slice(cc * lanes, (cc + 1) * lanes)
            sum_ = jnp.zeros((end - first_row, lanes), f32)
            for j in range(taps_n):
                start = first_row + lead - taps_n + 1 + j
                sum_ = sum_ + taps_ref[j : j + 1, cols] * glu[p, cc, pl.ds(start, end - first_row), :]
            into[first_row:end, cols] = sum_.astype(bf16)
            one = one + jnp.sum(sum_, axis=1, keepdims=True)
            two = two + jnp.sum(sum_ * sum_, axis=1, keepdims=True)
        return one, two

    ahead = (1, 3, 2)
    order = [(x + d) % 4 for d in ahead] + [x]

    def conv_to(k, first_row, end):
        return pltpu.make_async_remote_copy(
            src_ref=conv_send.at[k, pl.ds(first_row, end - first_row)],
            dst_ref=conv_recv.at[3 - ahead[k], pl.ds(first_row, end - first_row)],
            send_sem=conv_sem.at[3],
            recv_sem=conv_sem.at[3 - ahead[k]],
            device_id={"sp": sp, "tp": order[k]},
            device_id_type=MESH,
        )

    def stat_to(k):
        return pltpu.make_async_remote_copy(
            src_ref=stat_send.at[k],
            dst_ref=stat_recv.at[3 - ahead[k]],
            send_sem=stat_sem.at[0],
            recv_sem=stat_sem.at[1],
            device_id={"sp": sp, "tp": order[k]},
            device_id_type=MESH,
        )

    def gain_to(d):
        return pltpu.make_async_remote_copy(
            src_ref=channel_gain_ref,
            dst_ref=gains.at[3 - d],
            send_sem=gain_sem.at[0],
            recv_sem=gain_sem.at[1],
            device_id={"sp": sp, "tp": (x + d) % 4},
            device_id_type=MESH,
        )

    total_rows = value.shape[0]
    behind = {"sp": (sp + 1) % 32, "tp": x}
    rims = [
        pltpu.make_async_remote_copy(
            src_ref=ref.at[pl.ds(total_rows - lead, lead)],
            dst_ref=rim.at[i],
            send_sem=rim_sem.at[0],
            recv_sem=rim_sem.at[1],
            device_id=behind,
            device_id_type=MESH,
        )
        for i, ref in enumerate((value, gate_in))
    ]
    lower = [convolve(order[0], conv_send.at[0], lead, rows)]
    pl.semaphore_wait(barrier, len(met))
    for copy in rims:
        copy.start()
    conv_to(0, lead, rows).start()
    lower.append(convolve(order[1], conv_send.at[1], lead, rows))
    conv_to(1, lead, rows).start()
    lower.append(convolve(order[2], conv_send.at[2], lead, rows))
    small[0].wait()
    for d in range(1, 4):
        gain_to(d).start()
    spread_word(0, y_line)
    lower.append(convolve(x, conv_own, lead, rows))
    pltpu.make_async_copy(rim, rim, rim_sem.at[1]).wait()
    gated = rim[0].astype(f32) * (1.0 / (1.0 + jnp.exp(-rim[1].astype(f32))))
    put_glu(0, jnp.where(sp > 0, gated, jnp.zeros_like(gated)), 0)
    for k in range(3):
        upper = convolve(order[k], conv_send.at[k], 0, lead)
        for i in range(2):
            stat_send[k, i : i + 1, :] = along(jnp.concatenate([upper[i], lower[k][i]], axis=0))
        stat_to(k).start()
    conv_to(2, 0, rows).start()
    for k in range(2):
        conv_to(k, 0, lead).start()
    upper = convolve(x, conv_own, 0, lead)
    sums = [along(jnp.concatenate([upper[i], lower[3][i]], axis=0)) for i in range(2)]
    pl.semaphore_wait(word.at[0], 3)
    spread_word(1, z_line)
    for copy in small[1:]:
        copy.wait()

    row = [routes_ref[k : k + 1, :] for k in range(2)]
    col = [across(r) for r in row]
    r_id = lax.broadcasted_iota(jnp.int32, (rows, rows), 0)
    c_id = lax.broadcasted_iota(jnp.int32, (rows, rows), 1)
    every = r_id >= 0
    before_l = [
        slot_rows(row[0], col[0], r_id < c_id, 0),
        slot_rows(row[1], col[0], every, 0) + slot_rows(row[1], col[1], r_id < c_id, 0),
    ]
    before_s = [
        slot_rows(col[0], row[0], c_id < r_id, 1),
        slot_rows(col[1], row[0], every, 1) + slot_rows(col[1], row[1], c_id < r_id, 1),
    ]
    where_l = [offset_of(row[k]) * BLOCK + before_l[k] for k in range(2)]
    where_s = [offset_of(col[k]) * BLOCK + before_s[k] for k in range(2)]
    key_l = [jnp.concatenate([where_l[k] + q * SLOTS for q in range(QUARTERS)], axis=1) for k in range(2)]

    def choose(b, carry):
        ids = lax.broadcasted_iota(jnp.int32, (rows, PEERS * BLOCK), 1)
        k, q = b // QUARTERS, b % QUARTERS
        key = jnp.where(k == 0, where_s[0], where_s[1]) + q * SLOTS
        pick[pl.ds(pl.multiple_of(b * rows, rows), rows)] = (ids == key).astype(f32).astype(bf16)
        return carry

    lax.fori_loop(0, QUARTERS, choose, 0)
    pl.semaphore_wait(word.at[1], 3)
    spread_word(2, [twin])
    lax.fori_loop(QUARTERS, 2 * QUARTERS, choose, 0)

    pltpu.make_async_copy(gains, gains, gain_sem.at[1]).wait()
    pltpu.make_async_copy(stat_recv, stat_recv, stat_sem.at[1]).wait()
    for k in range(3):
        sums = [sums[i] + stat_recv[k, i : i + 1, :] for i in range(2)]
    middle = sums[0] / width
    spread = sums[1] / width - middle * middle
    scale = across(lax.rsqrt(spread + 1e-05))
    middle = across(middle)
    for copy in weights[:2]:
        copy.wait()
    for i in (0, 3, 1, 2):
        if i > 0:
            pltpu.make_async_copy(conv_recv.at[i - 1], conv_recv.at[i - 1], conv_sem.at[i - 1]).wait()
        values = conv_own[...] if i == 0 else conv_recv[i - 1]
        gain = channel_gain_ref[...] if i == 0 else gains[i - 1]
        act[...] = silu((values.astype(f32) - middle) * scale * gain).astype(bf16)
        block = (x + i) % 4

        for b in range(QUARTERS):
            cols = slice(b * quarter, (b + 1) * quarter)
            part = jnp.dot(
                act[...],
                point[pl.ds(pl.multiple_of(block * quarter, quarter), quarter), cols],
                preferred_element_type=f32,
            )
            h1[b] = (residual_scale * residual[:, cols].astype(f32) if i == 0 else h1[b]) + part
    middle = sum(jnp.sum(h1[q], axis=1, keepdims=True) for q in range(QUARTERS)) / width
    centred = [h1[q] - middle for q in range(QUARTERS)]
    spread = sum(jnp.sum(v * v, axis=1, keepdims=True) for v in centred) / width
    scale = lax.rsqrt(spread + 1e-05)
    for q in range(QUARTERS):
        cols = slice(q * quarter, (q + 1) * quarter)
        stacked[pl.ds(q * rows, rows), :] = (centred[q] * scale * first_gain_ref[:, cols]).astype(bf16)

    def fill(b, carry):
        ids = lax.broadcasted_iota(jnp.int32, (512, QUARTERS * rows), 0) + b * 512
        chosen = ((ids == key_l[0]) | (ids == key_l[1])).astype(f32).astype(bf16)
        picked = jnp.dot(chosen, stacked[...], preferred_element_type=f32).astype(bf16)
        send[pl.ds(pl.multiple_of(b * 32, 32), 32)] = picked.reshape(32, BLOCK, quarter)
        return carry

    pl.semaphore_wait(word.at[2], 1)
    def dispatch_to(n, h):
        return pltpu.make_async_remote_copy(
            src_ref=send.at[n],
            dst_ref=recv.at[n],
            send_sem=send_sem,
            recv_sem=recv_sem.at[h],
            device_id=partner(n, 1),
            device_id_type=MESH,
        )

    def answer_to(n, h):
        return pltpu.make_async_remote_copy(
            src_ref=back_send.at[n],
            dst_ref=back_recv.at[n],
            send_sem=back_send_sem,
            recv_sem=back_recv_sem.at[h],
            device_id=partner(n, -1),
            device_id_type=MESH,
        )

    recv_group = 512 // BLOCK
    for h, part in enumerate(PARTS):
        lax.fori_loop(part[0] // recv_group, sum(part) // recv_group, fill, 0)
        for n in far_to_near(part):
            dispatch_to(n, h).start()
    recv[0] = send[0]

    i = lax.broadcasted_iota(jnp.int32, (256, 256), 0)
    j = lax.broadcasted_iota(jnp.int32, (256, 256), 1)
    to_flat = (((i // 4) % 16) * 16 + (i // 64) * 4 + i % 4 == j).astype(f32).astype(bf16)
    to_block = (((j // 4) % 16) * 16 + (j // 64) * 4 + j % 4 == i).astype(f32).astype(bf16)

    for h, (start, count) in enumerate(PARTS):
        own = 1 if h == 0 else 0
        m = count * SLOTS
        landed = recv.at[pl.ds(start + own, count - own)]
        pltpu.make_async_copy(landed, landed, recv_sem.at[h]).wait()
        for g in range(count // 16):
            block = recv[pl.ds(start + g * 16, 16)].reshape(256, quarter)
            moved = jnp.dot(to_flat, block, preferred_element_type=f32).astype(bf16)
            for q in range(QUARTERS):
                flat[pl.ds(g * 64, 64), pl.ds(q * quarter, quarter)] = moved[q * 64 : (q + 1) * 64]
        if h == 0:
            for copy in weights[2:]:
                copy.wait()

        def hide(b, carry):
            cols = pl.ds(pl.multiple_of(b * 256, 256), 256)
            gate = jnp.dot(flat[:m], gate_w[:, cols], preferred_element_type=f32)
            upper = jnp.dot(flat[:m], up_w[:, cols], preferred_element_type=f32)
            hidden[:m, cols] = (silu(gate) * upper).astype(bf16)
            return carry

        lax.fori_loop(0, hidden.shape[1] // 256, hide, 0)
        for q in range(QUARTERS):
            cols = pl.ds(q * quarter, quarter)
            result = jnp.dot(hidden[:m], down_w[:, cols], preferred_element_type=f32).astype(bf16)
            for g in range(count // 16):
                answer[g, pl.ds(q * 64, 64), :] = result[g * 64 : (g + 1) * 64]
        for g in range(count // 16):
            moved = jnp.dot(to_block, answer[g], preferred_element_type=f32).astype(bf16)
            back_send[pl.ds(start + g * 16, 16)] = moved.reshape(16, BLOCK, quarter)
        if h == 0:
            back_recv[0] = back_send[0]
        for n in far_to_near((start, count)):
            answer_to(n, h).start()

    for h, (start, count) in enumerate(PARTS):
        own = 1 if h == 0 else 0
        landed = back_recv.at[pl.ds(start + own, count - own)]
        pltpu.make_async_copy(landed, landed, back_recv_sem.at[h]).wait()
        block = back_recv[pl.ds(start, count)].reshape(count * BLOCK, quarter)
        part = jnp.dot(pick[:, pl.ds(start * BLOCK, count * BLOCK)], block, preferred_element_type=f32)
        total[...] = part if h == 0 else total[...] + part

    share = [across(score_ref[k : k + 1, :] / (score_ref[0:1, :] + score_ref[1:2, :])) for k in range(2)]
    mixed = []
    for q in range(QUARTERS):
        base = residual_scale * stacked[pl.ds(q * rows, rows), :].astype(f32)
        one = total[pl.ds(q * rows, rows), :] * share[0]
        two = total[pl.ds((QUARTERS + q) * rows, rows), :] * share[1]
        mixed.append(base + (one + two))
    middle = sum(jnp.sum(m, axis=1, keepdims=True) for m in mixed) / width
    mixed = [m - middle for m in mixed]
    spread = sum(jnp.sum(m * m, axis=1, keepdims=True) for m in mixed) / width
    scale = lax.rsqrt(spread + 1e-05)
    for q in range(QUARTERS):
        cols = slice(q * quarter, (q + 1) * quarter)
        out_ref[:, cols] = (mixed[q] * scale * second_gain_ref[:, cols]).astype(bf16)

    for copy in rims:
        copy.wait_send()
    for k in range(3):
        conv_to(k, 0, rows).wait_send()
        stat_to(k).wait_send()
    for d in range(1, 4):
        gain_to(d).wait_send()
    sent = send.at[pl.ds(1, PEERS - 1)]
    pltpu.make_async_copy(sent, sent, send_sem).wait()
    sent = back_send.at[pl.ds(1, PEERS - 1)]
    pltpu.make_async_copy(sent, sent, back_send_sem).wait()


def per_device(
    conv_value,
    conv_gate,
    conv_taps,
    channel_gain,
    point_weight,
    residual_in,
    first_gain,
    second_gain,
    routes,
    route_score,
    expert_gate,
    expert_up,
    expert_down,
):
    rows, width = residual_in.shape
    inner = expert_gate.shape[2]
    tokens, quarter = conv_value.shape
    lanes = 128
    lead = -(-(conv_taps.shape[0] - 1) // 16) * 16
    vmem = pl.BlockSpec(memory_space=pltpu.VMEM)
    hbm = pl.BlockSpec(memory_space=pl.ANY)
    blocks = pltpu.VMEM((PEERS, BLOCK, quarter), bf16)
    dma = pltpu.SemaphoreType.DMA
    return pl.pallas_call(
        layer_kernel,
        out_shape=pltpu.VMEM((rows, width), bf16),
        in_specs=[hbm] * 13,
        out_specs=vmem,
        scratch_shapes=[
            pltpu.VMEM(conv_taps.shape, f32),
            pltpu.VMEM((1, quarter), f32),
            pltpu.VMEM((1, width), f32),
            pltpu.VMEM((1, width), f32),
            pltpu.VMEM((2, rows), jnp.int32),
            pltpu.VMEM((2, rows), f32),
            pltpu.VMEM((3, 2, rows), f32),
            pltpu.VMEM((3, 2, rows), f32),
            pltpu.VMEM((tokens, quarter), bf16),
            pltpu.VMEM((tokens, quarter), bf16),
            pltpu.VMEM((2, lead, quarter), bf16),
            pltpu.VMEM((4, quarter // lanes, lead + rows, lanes), f32),
            pltpu.VMEM((3, rows, quarter), bf16),
            pltpu.VMEM((rows, quarter), bf16),
            pltpu.VMEM((3, rows, quarter), bf16),
            pltpu.VMEM((3, 1, quarter), f32),
            pltpu.VMEM((width, width), bf16),
            pltpu.VMEM((rows, width), bf16),
            pltpu.VMEM((rows, quarter), bf16),
            pltpu.VMEM((QUARTERS, rows, quarter), f32),
            pltpu.VMEM((QUARTERS * rows, quarter), bf16),
            pltpu.VMEM((width, inner), bf16),
            pltpu.VMEM((width, inner), bf16),
            pltpu.VMEM((inner, width), bf16),
            blocks,
            blocks,
            pltpu.VMEM((HALF * SLOTS, width), bf16),
            pltpu.VMEM((HALF * SLOTS, inner), bf16),
            pltpu.VMEM((4, 256, quarter), bf16),
            blocks,
            blocks,
            pltpu.VMEM((2 * QUARTERS * rows, PEERS * BLOCK), bf16),
            pltpu.VMEM((2 * QUARTERS * rows, quarter), f32),
            dma((3,)),
            dma((5,)),
            dma((5,)),
            dma((2,)),
            dma((2,)),
            dma((2,)),
            dma((4,)),
            dma,
            dma((4,)),
            dma,
            dma((4,)),
            pltpu.SemaphoreType.REGULAR((3,)),
        ],
        compiler_params=pltpu.CompilerParams(
            collective_id=1, has_side_effects=True, vmem_limit_bytes=60 * 1024 * 1024
        ),
        name="layer",
    )(
        conv_value,
        conv_gate,
        conv_taps,
        channel_gain.reshape(1, -1),
        point_weight,
        residual_in,
        first_gain.reshape(1, -1),
        second_gain.reshape(1, -1),
        routes.T,
        route_score.T,
        expert_gate,
        expert_up,
        expert_down,
    )


def solution(mesh):
    in_specs = (
        P("sp", "tp"),
        P("sp", "tp"),
        P(None, "tp"),
        P("tp"),
        P(),
        P(("sp", "tp"), None),
        P(),
        P(),
        P(("sp", "tp"), None),
        P(("sp", "tp"), None),
        P(("sp", "tp"), None, None),
        P(("sp", "tp"), None, None),
        P(("sp", "tp"), None, None),
    )
    out_specs = P(("sp", "tp"), None)
    return jax.shard_map(
        per_device, mesh=mesh, in_specs=in_specs, out_specs=out_specs, check_vma=False
    )
```
